1024 devices in a mesh: sp: 128 (over z, y), tp: 8 (over x, core).
Axes of the slice: x: 4, y: 4, z: 32, core: 2. Of those that a mesh axis runs over, the one named last changes fastest.
Arguments:
- tokens: bfloat16 [4, 8192, 2048], P(None, ('sp', 'tp')), may hold values from -6 to 6
- in_gain: float32 [2048], replicated, may hold values from 0.1 to 1.9
- gate_weight: bfloat16 [2048, 1024], P(None, 'tp'), may hold values from -0.125 to 0.125
- input_weight: bfloat16 [2048, 1024], P(None, 'tp'), may hold values from -0.125 to 0.125
- key_weight: bfloat16 [2048, 512], P(None, 'tp'), may hold values from -0.125 to 0.125
- query_weight: bfloat16 [2048, 512], P(None, 'tp'), may hold values from -0.125 to 0.125
- step_weight: bfloat16 [2048, 16], replicated, may hold values from -0.125 to 0.125
- conv_input: float32 [4, 1024], P(None, 'tp'), may hold values from -3 to 3
- conv_key: float32 [4, 512], P(None, 'tp'), may hold values from -3 to 3
- conv_query: float32 [4, 512], P(None, 'tp'), may hold values from -3 to 3
- step_bias: float32 [16], P('tp'), may hold values from -5 to 1
- decay_rate: float32 [16], P('tp'), may hold values from 0 to 1, as said below
- decay_extra: float32 [4, 16, 8192], P(None, 'tp', 'sp'), may hold values from -0.7 to 0, as said below
- out_gain: float32 [1024], P('tp'), may hold values from 0.1 to 1.9
- out_weight: bfloat16 [1024, 2048], replicated, may hold values from -0.1875 to 0.1875
Outputs:
- output: bfloat16 [4, 8192, 2048], P(None, ('sp', 'tp'))
The draws below stay inside these ranges and needn't reach their ends.
Inputs may be any that keep to these rules, and one draw needn't show every extreme that they name: `decay_rate`: one positive rate a head. `decay_extra`: never positive.
All inputs are finite; a program needn't handle non-finite values.
Results may differ from the reference program's by a relative error of at most 0.0072.
Values may be sent and summed in bfloat16 or wider, within the bound.
A program may use at most 128 MiB of HBM per device.

```python
import jax
import jax.numpy as jnp
from jax import lax

D = 2048
HEAD_TOTAL = 16
HEAD_DIM = 64
GROUPS = 8
STATE = 64
CONV = 4
BLOCK = 64
SEQUENCE_TOTAL = 4
INNER = 1024
LEN = 8192


def fast_heads(key):
    picks = jax.random.randint(jax.random.fold_in(key, 7), (HEAD_TOTAL,), 0, 8)
    return picks < 4


def draw_decay_rate(key, part):
    is_fast = fast_heads(key)
    unit_draw = jax.random.uniform(jax.random.fold_in(key, 11), (HEAD_TOTAL,), jnp.float32)
    fast_rate = jnp.exp(jnp.log(1.0 / 60.0) + unit_draw * jnp.log(60.0 / 25.0))
    slow_rate = jnp.exp(jnp.log(8.0) + unit_draw * jnp.log(20.0 / 8.0)) / LEN
    return jnp.where(is_fast, fast_rate, slow_rate).astype(jnp.float32)


def draw_step_bias(key, part):
    is_fast = fast_heads(key)
    unit_draw = jax.random.uniform(jax.random.fold_in(key, 13), (HEAD_TOTAL,), jnp.float32)
    return jnp.where(is_fast, unit_draw - 0.5, unit_draw - 4.5).astype(jnp.float32)


def draw_decay_extra(key, part):
    block_total = LEN // BLOCK
    unit_draw = jax.random.uniform(jax.random.fold_in(key, 17), (SEQUENCE_TOTAL, HEAD_TOTAL, block_total), jnp.float32)
    factor = jnp.exp(jnp.log(0.1) + unit_draw * jnp.log(8.0)) / LEN
    block_displacement = -jnp.repeat(factor, BLOCK, axis=2)
    first_spot = jax.random.randint(jax.random.fold_in(key, 19), (SEQUENCE_TOTAL, HEAD_TOTAL, 1), 0, LEN)
    spot_offset = jax.random.randint(jax.random.fold_in(key, 29), (SEQUENCE_TOTAL, HEAD_TOTAL, 1), 1, LEN)
    second_spot = (first_spot + spot_offset) % LEN
    spots = jnp.concatenate([first_spot, second_spot], axis=2)
    segment_lengths = jax.random.uniform(jax.random.fold_in(key, 23), (SEQUENCE_TOTAL, HEAD_TOTAL, 2), jnp.float32, 0.22, 0.69)
    positions = jnp.arange(LEN)[None, None, :, None]
    matching_count = positions == spots[:, :, None, :]
    token_segments = jnp.sum(jnp.where(matching_count, segment_lengths[:, :, None, :], 0.0), axis=3)
    return (block_displacement - token_segments).astype(jnp.float32)


def shard_levels(rng, dims, shards, low, top_value):
    factor_of, own = 1.0, jax.random.fold_in(rng, 6)
    for dim, shards_of in shards:
        draws = jnp.exp(jax.random.uniform(jax.random.fold_in(own, dim), (shards_of,), jnp.float32, low / len(shards), top_value / len(shards)))
        factor_of = factor_of * jnp.repeat(draws, dims[dim] // shards_of).reshape([-1 if axis == dim else 1 for axis in range(len(dims))])
    return factor_of


def scatter_about(rng, extent, deviation, reach, pieces=(), dtype=jnp.bfloat16):
    values = deviation * jax.random.normal(rng, extent, jnp.float32)
    if pieces:
        values = values * shard_levels(rng, extent, pieces, -0.22, 0.18)
    return jnp.clip(values, -reach, reach).astype(dtype)


def setup_inputs(seed: int = 0) -> dict:
    key_of = jax.random.split(jax.random.key(seed), 16)
    return {
        "tokens": scatter_about(key_of[0], (SEQUENCE_TOTAL, LEN, D), 1.0, 6.0, ((1, 1024),)),
        "in_gain": jnp.clip(1.0 + 0.18 * jax.random.normal(key_of[1], (D,), jnp.float32), 0.1, 1.9),
        "gate_weight": scatter_about(key_of[2], (D, INNER), D ** -0.5, 0.125, ((1, 8),)),
        "input_weight": scatter_about(key_of[3], (D, INNER), D ** -0.5, 0.125, ((1, 8),)),
        "key_weight": scatter_about(key_of[4], (D, GROUPS * STATE), D ** -0.5, 0.125, ((1, 8),)),
        "query_weight": scatter_about(key_of[5], (D, GROUPS * STATE), D ** -0.5, 0.125, ((1, 8),)),
        "step_weight": scatter_about(key_of[6], (D, HEAD_TOTAL), D ** -0.5, 0.125),
        "conv_input": scatter_about(key_of[7], (CONV, INNER), CONV ** -0.5, 3.0, ((1, 8),), jnp.float32),
        "conv_key": scatter_about(key_of[8], (CONV, GROUPS * STATE), CONV ** -0.5, 3.0, ((1, 8),), jnp.float32),
        "conv_query": scatter_about(key_of[9], (CONV, GROUPS * STATE), CONV ** -0.5, 3.0, ((1, 8),), jnp.float32),
        "step_bias": draw_step_bias(jax.random.fold_in(key_of[15], 71), 0),
        "decay_rate": draw_decay_rate(jax.random.fold_in(key_of[15], 71), 0),
        "decay_extra": draw_decay_extra(jax.random.fold_in(key_of[15], 71), 0),
        "out_gain": jnp.clip(1.0 + 0.18 * jax.random.normal(key_of[13], (INNER,), jnp.float32), 0.1, 1.9),
        "out_weight": scatter_about(key_of[14], (INNER, D), INNER ** -0.5, 0.1875),
    }


NORM_EPS = 1e-06
PRECISE = lax.Precision.HIGHEST

def rms_rows(values, gain_row):
    mean_sq = lax.optimization_barrier(jnp.mean(values * values, axis=-1, keepdims=True))
    return values * lax.rsqrt(mean_sq + NORM_EPS) * gain_row

def causal_blend(rim_rows, local_rows, weights):
    length = local_rows.shape[1]
    padded = jnp.concatenate([rim_rows, local_rows], axis=1).astype(jnp.float32)
    summed_rows = padded[:, 0:length, :] * weights[0]
    for offset in range(1, weights.shape[0]):
        summed_rows = summed_rows + padded[:, offset:offset + length, :] * weights[offset]
    return jax.nn.silu(summed_rows)

def reference(tokens, in_gain, gate_weight, input_weight, key_weight, query_weight, step_weight, conv_input, conv_key, conv_query, step_bias, decay_rate, decay_extra, out_gain, out_weight):
    ratio_heads = HEAD_TOTAL // GROUPS
    normed = rms_rows(tokens.astype(jnp.float32), in_gain).astype(jnp.bfloat16)
    flat_rows = normed.reshape(SEQUENCE_TOTAL * LEN, D)

    def project(weight_matrix):
        result = jnp.dot(flat_rows, weight_matrix, preferred_element_type=jnp.float32)
        return result.astype(jnp.bfloat16).reshape(SEQUENCE_TOTAL, LEN, weight_matrix.shape[1])
    gate_in = project(gate_weight)
    input_in = project(input_weight)
    key_in = project(key_weight)
    query_in = project(query_weight)
    step_in = project(step_weight)
    rim_inner = jnp.zeros((SEQUENCE_TOTAL, CONV - 1, INNER), jnp.bfloat16)
    rim_state = jnp.zeros((SEQUENCE_TOTAL, CONV - 1, GROUPS * STATE), jnp.bfloat16)
    conv_values = causal_blend(rim_inner, input_in, conv_input)
    conv_keys = causal_blend(rim_state, key_in, conv_key)
    conv_queries = causal_blend(rim_state, query_in, conv_query)
    step_size = jax.nn.softplus(step_in.astype(jnp.float32) + step_bias)
    log_decay = -step_size * decay_rate + jnp.transpose(decay_extra, (0, 2, 1))
    block_count = LEN // BLOCK

    def to_blocks(tensor):
        shaped = tensor.reshape((SEQUENCE_TOTAL, block_count, BLOCK) + tensor.shape[2:])
        return jnp.moveaxis(shaped, 1, 0)
    x_blocks = to_blocks(conv_values.reshape(SEQUENCE_TOTAL, LEN, HEAD_TOTAL, HEAD_DIM) * step_size[..., None])
    b_blocks = to_blocks(conv_keys.reshape(SEQUENCE_TOTAL, LEN, GROUPS, STATE))
    c_blocks = to_blocks(conv_queries.reshape(SEQUENCE_TOTAL, LEN, GROUPS, STATE))
    d_blocks = to_blocks(log_decay)
    causal = jnp.tril(jnp.ones((BLOCK, BLOCK), bool))[None, :, :, None]

    def block_step(passed_recurrence, inputs):
        x_now, b_now, c_now, d_now = inputs
        inside_block = jnp.cumsum(d_now, axis=1)
        spread_log = inside_block[:, :, None, :] - inside_block[:, None, :, :]
        decay_matrix = jnp.where(causal, jnp.exp(jnp.where(causal, spread_log, 0.0)), 0.0)
        scores = jnp.einsum('slgn,stgn->sltg', c_now, b_now, precision=PRECISE)
        scores = jnp.repeat(scores, ratio_heads, axis=3)
        key_heads = jnp.repeat(b_now, ratio_heads, axis=2)
        query_heads = jnp.repeat(c_now, ratio_heads, axis=2)
        inner_part = jnp.einsum('slth,sthp->slhp', scores * decay_matrix, x_now, precision=PRECISE)
        forwarded_portion = jnp.einsum('slhn,shpn->slhp', query_heads, passed_recurrence, precision=PRECISE)
        forwarded_portion = forwarded_portion * jnp.exp(inside_block)[..., None]
        tail_weight = jnp.exp(inside_block[:, -1:, :] - inside_block)
        fresh = jnp.einsum('slhn,slhp->shpn', key_heads, x_now * tail_weight[..., None], precision=PRECISE)
        next_state = jnp.exp(inside_block[:, -1, :])[:, :, None, None] * passed_recurrence + fresh
        return (next_state, inner_part + forwarded_portion)
    start_state = jnp.zeros((SEQUENCE_TOTAL, HEAD_TOTAL, HEAD_DIM, STATE), jnp.float32)
    _, out_blocks = lax.scan(block_step, start_state, (x_blocks, b_blocks, c_blocks, d_blocks))
    heads_out = jnp.moveaxis(out_blocks, 0, 1).reshape(SEQUENCE_TOTAL, LEN, INNER)
    gated = heads_out * jax.nn.silu(gate_in.astype(jnp.float32))
    group_width = ratio_heads * HEAD_DIM
    mixed = rms_rows(gated.reshape(SEQUENCE_TOTAL, LEN, GROUPS, group_width), out_gain.reshape(GROUPS, group_width))
    mixed = mixed.reshape(SEQUENCE_TOTAL * LEN, INNER).astype(jnp.bfloat16)
    output = jnp.dot(mixed, out_weight, preferred_element_type=jnp.float32).astype(jnp.bfloat16)
    return output.reshape(SEQUENCE_TOTAL, LEN, D)
```

```python
import functools

import jax
import jax.numpy as jnp
from jax import lax
from jax.experimental import pallas as pl
from jax.experimental.pallas import tpu as pltpu
from jax.sharding import PartitionSpec as P

HEAD_TOTAL = 16
HEAD_DIM = 64
GROUPS = 8
STATE = 64
CONV = 4
BLOCK = 64


NORM_EPS = 1e-06
PRECISE = lax.Precision.HIGHEST


def in_order(tiles, dim):
    tiles = jnp.moveaxis(tiles, 0, dim)
    lengths = tiles.shape
    return tiles.reshape(*lengths[:dim], lengths[dim] * lengths[dim + 1], *lengths[dim + 2 :])


def from_everyone(array, axis):
    length = lax.axis_size(axis)
    return lax.all_to_all(
        jnp.broadcast_to(array[None], (length, *array.shape)), axis, 0, 0, tiled=True
    )


def collect(array, axis, dim):
    return in_order(from_everyone(array, axis), dim)


def from_behind(array, axis, by):
    length = lax.axis_size(axis)
    pairs = [(i, i + by) for i in range(length) if 0 <= i + by < length]
    return lax.ppermute(array, axis, pairs)


MEMBERS = 16
MESH = pl.DeviceIdType.MESH


def scan_kernel(
    blocks, state_ref, logs_ref, out_ref,
    chunk_send, chunk_recv, log_recv, part_sums, part_logs,
    total_send, total_log, total_recv, total_log_recv, back_send,
    sem_c, sem_l, sem_t, sem_tl, sem_b,
):
    sp = lax.axis_index("sp")
    block, me = sp // MEMBERS, sp % MEMBERS

    def remote(source, target, sems, slot_here, slot_there, device):
        return pltpu.make_async_remote_copy(
            src_ref=source,
            dst_ref=target,
            send_sem=sems.at[0, slot_here],
            recv_sem=sems.at[1, slot_there],
            device_id={"sp": device},
            device_id_type=MESH,
        )

    for k in range(blocks - 1):
        total_recv[k] = jnp.zeros((16, 128), jnp.bfloat16)
        total_log_recv[k] = jnp.zeros((1, 128), jnp.float32)
    for c in range(MEMBERS):
        chunk_send[c] = state_ref[c * 16 : (c + 1) * 16, :].astype(jnp.bfloat16)

    barrier = pltpu.get_barrier_semaphore()
    for k in range(1, MEMBERS):
        pl.semaphore_signal(
            barrier, inc=1, device_id={"sp": block * MEMBERS + (me + k) % MEMBERS},
            device_id_type=MESH,
        )
    for k in range(1, blocks):
        pl.semaphore_signal(
            barrier, inc=1, device_id={"sp": ((block + k) % blocks) * MEMBERS + me},
            device_id_type=MESH,
        )
    pl.semaphore_wait(barrier, MEMBERS + blocks - 2)

    sends = []
    for k in range(1, MEMBERS):
        peer = (me + k) % MEMBERS
        device = block * MEMBERS + peer
        one = remote(logs_ref.at[peer // 4], log_recv.at[me], sem_l, peer, me, device)
        one.start()
        two = remote(chunk_send.at[peer], chunk_recv.at[me], sem_c, peer, me, device)
        two.start()
        sends += [one, two]
    chunk_recv[me] = chunk_send[me]
    log_recv[me] = logs_ref[me // 4]
    for k in range(1, MEMBERS):
        peer = (me + k) % MEMBERS
        device = block * MEMBERS + peer
        remote(logs_ref.at[0], log_recv.at[peer], sem_l, me, peer, device).wait_recv()
        remote(chunk_send.at[0], chunk_recv.at[peer], sem_c, me, peer, device).wait_recv()

    running = jnp.zeros((16, 128), jnp.float32)
    log_sum = jnp.zeros((1, 128), jnp.float32)
    for m in range(MEMBERS):
        part_sums[m] = running
        part_logs[m] = log_sum
        here = log_recv[m]
        running = jnp.exp(here) * running + chunk_recv[m].astype(jnp.float32)
        log_sum = log_sum + here
    total_send[...] = running.astype(jnp.bfloat16)
    total_log[...] = log_sum

    def far(k, device):
        return (
            remote(total_log, total_log_recv.at[k - 1], sem_tl, k - 1, k - 1, device),
            remote(total_send, total_recv.at[k - 1], sem_t, k - 1, k - 1, device),
        )

    for k in range(1, blocks):
        @pl.when(block + k < blocks)
        def _():
            for copy in far(k, sp + k * MEMBERS):
                copy.start()
    for k in range(1, blocks):
        @pl.when(block >= k)
        def _():
            for copy in far(k, sp - k * MEMBERS):
                copy.wait_recv()
    incoming = jnp.zeros((16, 128), jnp.float32)
    for k in range(blocks - 1, 0, -1):
        incoming = jnp.exp(total_log_recv[k - 1]) * incoming + total_recv[k - 1].astype(jnp.float32)
    for m in range(MEMBERS):
        back_send[m] = (part_sums[m] + jnp.exp(part_logs[m]) * incoming).astype(jnp.bfloat16)
    for k in range(1, MEMBERS):
        peer = (me + k) % MEMBERS
        copy = remote(
            back_send.at[peer], out_ref.at[me], sem_b, peer, me, block * MEMBERS + peer
        )
        copy.start()
        sends.append(copy)
    out_ref[me] = back_send[me]
    for k in range(1, MEMBERS):
        peer = (me + k) % MEMBERS
        remote(
            back_send.at[0], out_ref.at[peer], sem_b, me, peer, block * MEMBERS + peer
        ).wait_recv()
    for copy in sends:
        copy.wait_send()
    for k in range(1, blocks):
        @pl.when(block + k < blocks)
        def _():
            for copy in far(k, sp + k * MEMBERS):
                copy.wait_send()


def states_before(state, logs):
    blocks = lax.axis_size("sp") // MEMBERS
    vmem = pl.BlockSpec(memory_space=pltpu.VMEM)
    return pl.pallas_call(
        functools.partial(scan_kernel, blocks),
        out_shape=jax.ShapeDtypeStruct((MEMBERS, 16, 128), jnp.bfloat16),
        in_specs=[vmem, vmem],
        out_specs=vmem,
        scratch_shapes=[
            pltpu.VMEM((MEMBERS, 16, 128), jnp.bfloat16),
            pltpu.VMEM((MEMBERS, 16, 128), jnp.bfloat16),
            pltpu.VMEM((MEMBERS, 1, 128), jnp.float32),
            pltpu.VMEM((MEMBERS, 16, 128), jnp.float32),
            pltpu.VMEM((MEMBERS, 1, 128), jnp.float32),
            pltpu.VMEM((16, 128), jnp.bfloat16),
            pltpu.VMEM((1, 128), jnp.float32),
            pltpu.VMEM((blocks - 1, 16, 128), jnp.bfloat16),
            pltpu.VMEM((blocks - 1, 1, 128), jnp.float32),
            pltpu.VMEM((MEMBERS, 16, 128), jnp.bfloat16),
            pltpu.SemaphoreType.DMA((2, MEMBERS)),
            pltpu.SemaphoreType.DMA((2, MEMBERS)),
            pltpu.SemaphoreType.DMA((2, blocks)),
            pltpu.SemaphoreType.DMA((2, blocks)),
            pltpu.SemaphoreType.DMA((2, MEMBERS)),
        ],
        compiler_params=pltpu.CompilerParams(collective_id=0, has_side_effects=True),
    )(state, logs)


def rms_rows(values, gain_row):
    mean_sq = jnp.mean(values * values, axis=-1, keepdims=True)
    return values * lax.rsqrt(mean_sq + NORM_EPS) * gain_row


def causal_blend(rim_rows, local_rows, weights):
    length = local_rows.shape[1]
    padded = jnp.concatenate([rim_rows, local_rows], axis=1).astype(jnp.float32)
    summed_rows = padded[:, 0:length, :] * weights[0]
    for offset in range(1, weights.shape[0]):
        summed_rows = summed_rows + padded[:, offset : offset + length, :] * weights[offset]
    return jax.nn.silu(summed_rows)


def local_pass(scaled_x, keys_b, readout_vectors, log_decay):
    seq_count, seg_len, heads_here = (scaled_x.shape[0], scaled_x.shape[1], scaled_x.shape[2])
    blocks_here = seg_len // BLOCK
    ratio_heads = HEAD_TOTAL // GROUPS

    def to_blocks(tensor):
        return tensor.reshape((seq_count, blocks_here, BLOCK) + tensor.shape[2:])

    x_blocks = to_blocks(scaled_x)
    b_blocks = to_blocks(keys_b)
    c_blocks = to_blocks(readout_vectors)
    inside_block = jnp.cumsum(to_blocks(log_decay), axis=2)
    causal = jnp.tril(jnp.ones((BLOCK, BLOCK), bool))[None, None, :, :, None]
    spread_log = inside_block[:, :, :, None, :] - inside_block[:, :, None, :, :]
    decay_matrix = jnp.where(causal, jnp.exp(jnp.where(causal, spread_log, 0.0)), 0.0)
    scores = jnp.einsum("sblgn,sbtgn->sbltg", c_blocks, b_blocks, precision=PRECISE)
    scores = jnp.repeat(scores, ratio_heads, axis=4)
    key_heads = jnp.repeat(b_blocks, ratio_heads, axis=3)
    query_heads = jnp.repeat(c_blocks, ratio_heads, axis=3)
    inner_part = jnp.einsum(
        "sblth,sbthp->sblhp", scores * decay_matrix, x_blocks, precision=PRECISE
    )
    tail_weight = jnp.exp(inside_block[:, :, -1:, :] - inside_block)
    block_states = jnp.einsum(
        "sblhn,sblhp->sbnhp", key_heads, x_blocks * tail_weight[..., None], precision=PRECISE
    )
    block_totals = inside_block[:, :, -1, :]
    local_out = inner_part.reshape(seq_count, seg_len, heads_here, HEAD_DIM)
    logs = jnp.repeat(jnp.sum(block_totals, axis=1), HEAD_DIM, axis=1)
    running = block_states.reshape(seq_count * STATE, heads_here * HEAD_DIM)
    prefix_log = jnp.cumsum(log_decay, axis=1)
    return (local_out, logs[:, None, :], running, prefix_log)


def read_in(local_out, readout_vectors, prefix_log, incoming):
    query_heads = jnp.repeat(readout_vectors, HEAD_TOTAL // GROUPS, axis=2)
    carried = jnp.einsum("slhn,snhp->slhp", query_heads, incoming, precision=PRECISE)
    return local_out + carried * jnp.exp(prefix_log)[..., None]


def body(
    tokens,
    in_gain,
    gate_weight,
    input_weight,
    key_weight,
    query_weight,
    step_weight,
    conv_input,
    conv_key,
    conv_query,
    step_bias,
    decay_rate,
    decay_extra,
    out_gain,
    out_weight,
):
    normed = rms_rows(tokens.astype(jnp.float32), in_gain).astype(jnp.bfloat16)
    joined_weight = jnp.concatenate(
        [gate_weight, input_weight, key_weight, query_weight, step_weight], axis=1
    )
    token_segment = collect(normed, "tp", 1)
    seq_count = token_segment.shape[0]
    row_count = token_segment.shape[1]
    result = jnp.dot(
        token_segment.reshape(seq_count * row_count, token_segment.shape[2]),
        joined_weight,
        preferred_element_type=jnp.float32,
    )
    projected = result.astype(jnp.bfloat16).reshape(seq_count, row_count, joined_weight.shape[1])
    seq_count, seg_len = (projected.shape[0], projected.shape[1])
    inner_here = gate_weight.shape[1]
    state_cols = key_weight.shape[1]
    heads_here = step_bias.shape[0]
    gate_in = projected[:, :, :inner_here]
    conv_in = projected[:, :, inner_here : 2 * inner_here + 2 * state_cols]
    step_all = projected[:, :, 2 * inner_here + 2 * state_cols :]
    rim_rows = from_behind(conv_in[:, seg_len - CONV + 1 :, :], "sp", 1)
    conv_weights = jnp.concatenate([conv_input, conv_key, conv_query], axis=1)
    conv_out = causal_blend(rim_rows, conv_in, conv_weights)
    conv_values = conv_out[:, :, :inner_here].reshape(seq_count, seg_len, heads_here, HEAD_DIM)
    keys_b = conv_out[:, :, inner_here : inner_here + state_cols].reshape(
        seq_count, seg_len, state_cols // STATE, STATE
    )
    readout_vectors = conv_out[:, :, inner_here + state_cols :].reshape(
        seq_count, seg_len, state_cols // STATE, STATE
    )
    own_steps = lax.dynamic_slice_in_dim(step_all, lax.axis_index("tp") * heads_here, heads_here, 2)
    step_size = jax.nn.softplus(own_steps.astype(jnp.float32) + step_bias)
    log_decay = -step_size * decay_rate + jnp.transpose(decay_extra, (0, 2, 1))
    scaled_x = conv_values * step_size[..., None]
    local_out, logs, final_state, prefix_log = local_pass(
        scaled_x, keys_b, readout_vectors, log_decay
    )
    incoming = states_before(final_state, logs)
    incoming = incoming.reshape(seq_count, STATE, heads_here, HEAD_DIM).astype(jnp.float32)
    blended_heads = read_in(local_out, readout_vectors, prefix_log, incoming)
    gated_rows = blended_heads.reshape(seq_count, seg_len, inner_here) * jax.nn.silu(
        gate_in.astype(jnp.float32)
    )
    group_width = HEAD_TOTAL // GROUPS * HEAD_DIM
    groups_here = inner_here // group_width
    normed_out = rms_rows(
        gated_rows.reshape(seq_count, seg_len, groups_here, group_width),
        out_gain.reshape(groups_here, group_width),
    )
    normed_out = normed_out.reshape(seq_count, seg_len, inner_here).astype(jnp.bfloat16)
    token_rows = lax.all_to_all(normed_out, "tp", split_axis=1, concat_axis=2, tiled=True)
    result = jnp.dot(
        token_rows.reshape(token_rows.shape[0] * token_rows.shape[1], token_rows.shape[2]),
        out_weight,
        preferred_element_type=jnp.float32,
    )
    return result.astype(jnp.bfloat16).reshape(
        token_rows.shape[0], token_rows.shape[1], out_weight.shape[1]
    )


def solution(mesh):
    placed = (
        P(None, ("sp", "tp"), None),
        P(),
        P(None, "tp"),
        P(None, "tp"),
        P(None, "tp"),
        P(None, "tp"),
        P(),
        P(None, "tp"),
        P(None, "tp"),
        P(None, "tp"),
        P("tp"),
        P("tp"),
        P(None, "tp", "sp"),
        P("tp"),
        P(),
    )
    return jax.shard_map(
        body, mesh=mesh, in_specs=placed, out_specs=P(None, ("sp", "tp"), None), check_vma=False
    )
```

```python
import functools

import jax
import jax.numpy as jnp
from jax import lax
from jax.experimental import pallas as pl
from jax.experimental.pallas import tpu as pltpu
from jax.sharding import PartitionSpec as P

STATE = 64
NORM_EPS = 1e-06
PRECISE = lax.Precision.HIGHEST
MEMBERS = 16
MESH = pl.DeviceIdType.MESH
F32 = jnp.float32
BF16 = jnp.bfloat16


def rounded(values):
    return values.astype(BF16).astype(F32)


def two_parts(values):
    high = values.astype(BF16)
    return high, (values - high.astype(F32)).astype(BF16)


def three_parts(values):
    high = values.astype(BF16)
    rest = values - high.astype(F32)
    middle = rest.astype(BF16)
    return high, middle, (rest - middle.astype(F32)).astype(BF16)


def silu(values):
    return values / (1.0 + jnp.exp(-values))


def softplus(values):
    return jnp.maximum(values, 0.0) + jnp.log1p(jnp.exp(-jnp.abs(values)))


def dot(a, b, contract=((1,), (0,)), precision=None):
    return lax.dot_general(
        a, b, (contract, ((), ())), precision=precision, preferred_element_type=F32
    )


def mixer_kernel(
    places, seqs,
    tokens_ref, gain_ref, gate_ref, input_ref, key_ref, query_ref, step_ref,
    conv_x_ref, conv_k_ref, conv_q_ref, bias_ref, rate_ref, extra_ref, out_gain_ref, out_w_ref,
    out_ref,
    tok, w_gi, w_kq, w_step, w_out, rows_in,
    gate_s, x_pad, kq_pad, step_s, extra_s,
    xs_s, kq_s, cum_s, inner_s, query_s,
    rim_send, rim_recv,
    chunk_send, chunk_recv, log_send, log_recv, part_sums, part_logs,
    total_send, total_log, total_recv, total_log_recv, back_send, back_recv,
    mix_send, mix_recv,
    sem_load, sem_gs, sem_gr, sem_rim, sem_c, sem_l, sem_t, sem_tl, sem_b, sem_m,
):
    blocks = places // MEMBERS
    sp, tp = lax.axis_index("sp"), lax.axis_index("tp")
    block, me = sp // MEMBERS, sp % MEMBERS
    chip, core = tp // 2, tp % 2
    ahead, behind = ((chip + 1) % 4) * 2 + core, ((chip + 3) % 4) * 2 + core
    partner = chip * 2 + 1 - core

    def load(k, source, target):
        copy = pltpu.make_async_copy(source, target, sem_load.at[k])
        copy.start()
        return copy

    tok_load = load(0, tokens_ref, tok)
    weight_loads = [
        load(1, gate_ref, w_gi.at[:, 0:128]),
        load(2, input_ref, w_gi.at[:, 128:256]),
        load(3, key_ref, w_kq.at[0:64, :]),
        load(4, query_ref, w_kq.at[64:128, :]),
    ]
    step_load = load(5, step_ref, w_step)
    out_load = load(6, out_w_ref, w_out)

    def remote(source, target, send_sem, recv_sem, **device):
        return pltpu.make_async_remote_copy(
            src_ref=source, dst_ref=target, send_sem=send_sem, recv_sem=recv_sem,
            device_id=device, device_id_type=MESH,
        )

    def pair(source, target, sems, here, there, device):
        return remote(source, target, sems.at[0, here], sems.at[1, there], sp=device)

    for k in range(blocks - 1):
        total_recv[k] = jnp.zeros((16, 128), BF16)
        total_log_recv[k] = jnp.zeros((1, 128), F32)

    @pl.when(sp == 0)
    def _():
        rim_recv[...] = jnp.zeros_like(rim_recv)

    barrier = pltpu.get_barrier_semaphore()

    def greet(**device):
        pl.semaphore_signal(barrier, inc=1, device_id=device, device_id_type=MESH)

    for k in range(1, 8):
        greet(tp=(tp + k) % 8)
    for k in range(1, MEMBERS):
        greet(sp=block * MEMBERS + (me + k) % MEMBERS)
    for k in range(1, blocks):
        greet(sp=((block + k) % blocks) * MEMBERS + me)
    greet(sp=(sp + 1) % places)
    greet(sp=(sp + places - 1) % places)

    tok_load.wait()
    values = tok[...].astype(F32).reshape(seqs * 8, tok.shape[2])
    mean_sq = jnp.mean(values * values, axis=-1, keepdims=True)
    rows_in[0] = (values * lax.rsqrt(mean_sq + NORM_EPS) * gain_ref[...]).astype(BF16)

    pl.semaphore_wait(barrier, 7 + MEMBERS - 1 + blocks - 1 + 2)

    gather_sends = []

    def pass_on(k, slot, half, to_slot, device):
        part = pl.ds(half * 16, 16)
        copy = remote(
            rows_in.at[slot, part], rows_in.at[to_slot, part],
            sem_gs.at[k], sem_gr.at[to_slot, half], tp=device,
        )
        copy.start()
        gather_sends.append(copy)

    def arrived(slot, half):
        part = pl.ds(half * 16, 16)
        remote(
            rows_in.at[slot, part], rows_in.at[slot, part],
            sem_gs.at[0], sem_gr.at[slot, half], tp=partner,
        ).wait_recv()

    pass_on(0, 0, 0, 4, ahead)
    pass_on(1, 0, 1, 2, behind)
    pass_on(2, 0, 1, 4, ahead)
    pass_on(3, 0, 0, 2, behind)
    pass_on(4, 0, 0, 1, partner)
    pass_on(5, 0, 1, 1, partner)

    row = lax.broadcasted_iota(jnp.int32, (64, 128), 0)
    lane = lax.broadcasted_iota(jnp.int32, (64, 128), 1)
    inside = lane % 64
    diagonal = row == inside
    causal = row >= inside
    first_head = lane < 64
    lane_row = lax.broadcasted_iota(jnp.int32, (1, 128), 1)
    bias_row = jnp.where(lane_row < 64, bias_ref[0], bias_ref[1])
    rate_row = jnp.where(lane_row < 64, rate_ref[0], rate_ref[1])

    step_load.wait()
    pick_row = lax.broadcasted_iota(jnp.int32, (128, 16), 0) // 64 + 2 * tp
    pick = (pick_row == lax.broadcasted_iota(jnp.int32, (128, 16), 1)).astype(F32).astype(BF16)
    w_kq[128:256, :] = dot(pick, w_step[...]).astype(BF16)
    same_head = (
        lax.broadcasted_iota(jnp.int32, (128, 128), 0) // 64
        == lax.broadcasted_iota(jnp.int32, (128, 128), 1) // 64
    ).astype(F32)
    for s in range(seqs):
        extra_row = jnp.concatenate([extra_ref[s, 0:1, :], extra_ref[s, 1:2, :]], axis=1)
        extra_s[s] = dot(jnp.where(diagonal, extra_row, 0.0), same_head, precision=PRECISE)
    for copy in weight_loads:
        copy.wait()

    arrived(4, 0)
    pass_on(6, 4, 0, 6, ahead)
    pass_on(7, 4, 0, 5, partner)
    arrived(2, 1)
    pass_on(8, 2, 1, 6, behind)
    pass_on(9, 2, 1, 3, partner)
    arrived(4, 1)
    pass_on(10, 4, 1, 5, partner)
    arrived(2, 0)
    pass_on(11, 2, 0, 3, partner)
    arrived(6, 0)
    pass_on(12, 6, 0, 7, partner)
    arrived(6, 1)
    pass_on(13, 6, 1, 7, partner)
    for slot in (1, 3, 5):
        arrived(slot, 0)
        arrived(slot, 1)

    position = [
        ((chip + away) % 4) * 2 + (core if same else 1 - core)
        for away in (0, 1, 3, 2)
        for same in (True, False)
    ]

    def project(first, count):
        rows = rows_in[first : first + count].reshape(count * 32, rows_in.shape[2])
        gate_x = rounded(dot(rows, w_gi[...]))
        kq_step = rounded(dot(rows, w_kq[...], ((1,), (1,))))
        for i in range(count):
            at = pl.multiple_of(position[first + i] * 8, 8)
            for s in range(seqs):
                part = slice(i * 32 + s * 8, i * 32 + s * 8 + 8)
                gate_s[s, pl.ds(at, 8), :] = gate_x[part, 0:128]
                x_pad[s, pl.ds(at + 8, 8), :] = gate_x[part, 128:256]
                kq_pad[s, pl.ds(at + 8, 8), :] = kq_step[part, 0:128]
                step_s[s, pl.ds(at, 8), :] = kq_step[part, 128:256]

    project(0, 6)
    arrived(7, 0)
    arrived(7, 1)
    project(6, 2)

    for i, padded in enumerate((x_pad, kq_pad)):
        tails = [padded[s, 64:72, :] for s in range(seqs)]
        rim_send[i] = jnp.concatenate(tails, axis=0).astype(BF16)

    def rim(device):
        return remote(rim_send, rim_recv, sem_rim.at[0], sem_rim.at[1], sp=device)

    @pl.when(sp + 1 < places)
    def _():
        rim(sp + 1).start()

    triangle = (
        lax.broadcasted_iota(jnp.int32, (64, 192), 0)
        >= lax.broadcasted_iota(jnp.int32, (64, 192), 1) % 64
    ).astype(F32).astype(BF16)
    for s in range(seqs):
        step = softplus(step_s[s] + bias_row)
        step_s[s] = step
        log_decay = extra_s[s] - step * rate_row
        cum = dot(triangle, jnp.concatenate(three_parts(log_decay), axis=0))
        cum_s[s] = cum
        log_send[s] = cum[63:64, :]

    @pl.when(sp > 0)
    def _():
        rim(sp - 1).wait_recv()

    conv_kq = jnp.concatenate([conv_k_ref[...], conv_q_ref[...]], axis=1)
    rim_x, rim_kq = rim_recv[0].astype(F32), rim_recv[1].astype(F32)
    for s in range(seqs):
        x_pad[s, 0:8, :] = rim_x[s * 8 : s * 8 + 8, :]
        kq_pad[s, 0:8, :] = rim_kq[s * 8 : s * 8 + 8, :]
        x_sum = x_pad[s, 5:69, :] * conv_x_ref[0:1, :]
        kq_sum = kq_pad[s, 5:69, :] * conv_kq[0:1, :]
        for k in range(1, 4):
            x_sum = x_sum + x_pad[s, 5 + k : 69 + k, :] * conv_x_ref[k : k + 1, :]
            kq_sum = kq_sum + kq_pad[s, 5 + k : 69 + k, :] * conv_kq[k : k + 1, :]
        scaled = silu(x_sum) * step_s[s]
        kq = silu(kq_sum)
        xs_s[s] = scaled
        kq_s[s] = kq
        cum = cum_s[s]
        x_high, x_low = two_parts(scaled * jnp.exp(cum[63:64, :] - cum))
        k_high, k_low = two_parts(kq[:, 0:64])
        state = dot(
            jnp.concatenate([k_high, k_high, k_low], axis=0),
            jnp.concatenate([x_high, x_low, x_high], axis=0),
            ((0,), (0,)),
        )
        for q in range(4):
            chunk_send[s * 4 + q] = state[q * 16 : q * 16 + 16, :].astype(BF16)

    sends = []
    for k in range(1, MEMBERS):
        peer = (me + k) % MEMBERS
        device = block * MEMBERS + peer
        one = pair(log_send.at[peer // 4], log_recv.at[me], sem_l, peer, me, device)
        one.start()
        two = pair(chunk_send.at[peer], chunk_recv.at[me], sem_c, peer, me, device)
        two.start()
        sends += [one, two]
    chunk_recv[me] = chunk_send[me]
    log_recv[me] = log_send[me // 4]

    for s in range(seqs):
        cum, kq, scaled = cum_s[s], kq_s[s], xs_s[s]
        keys, queries = kq[:, 0:64], kq[:, 64:128]
        query_s[s] = jnp.concatenate(two_parts(queries), axis=1)
        cum_row = jnp.sum(jnp.where(diagonal, cum, 0.0), axis=0, keepdims=True)
        decay = jnp.where(causal, jnp.exp(jnp.where(causal, cum - cum_row, 0.0)), 0.0)
        scores = dot(queries, jnp.concatenate([keys, keys], axis=0), ((1,), (1,)), PRECISE)
        apart = jnp.concatenate(
            [jnp.where(first_head, scaled, 0.0), jnp.where(first_head, 0.0, scaled)], axis=0
        )
        inner_s[s] = dot(scores * decay, apart, precision=PRECISE)
        cum_s[s] = jnp.exp(cum)
        gate_s[s] = silu(gate_s[s])

    for k in range(1, MEMBERS):
        peer = (me + k) % MEMBERS
        device = block * MEMBERS + peer
        pair(log_send.at[0], log_recv.at[peer], sem_l, me, peer, device).wait_recv()
        pair(chunk_send.at[0], chunk_recv.at[peer], sem_c, me, peer, device).wait_recv()

    running = jnp.zeros((16, 128), F32)
    log_sum = jnp.zeros((1, 128), F32)
    for m in range(MEMBERS):
        part_sums[m] = running
        part_logs[m] = log_sum
        here = log_recv[m]
        running = jnp.exp(here) * running + chunk_recv[m].astype(F32)
        log_sum = log_sum + here
    total_send[...] = running.astype(BF16)
    total_log[...] = log_sum

    def far(k, device):
        return (
            pair(total_log, total_log_recv.at[k - 1], sem_tl, k - 1, k - 1, device),
            pair(total_send, total_recv.at[k - 1], sem_t, k - 1, k - 1, device),
        )

    for k in range(1, blocks):
        @pl.when(block + k < blocks)
        def _():
            for copy in far(k, sp + k * MEMBERS):
                copy.start()
    for m in range(MEMBERS):
        part_logs[m] = jnp.exp(part_logs[m])
    out_load.wait()
    for k in range(1, blocks):
        @pl.when(block >= k)
        def _():
            for copy in far(k, sp - k * MEMBERS):
                copy.wait_recv()
    incoming = jnp.zeros((16, 128), F32)
    for k in range(blocks - 1, 0, -1):
        incoming = jnp.exp(total_log_recv[k - 1]) * incoming + total_recv[k - 1].astype(F32)
    for m in range(MEMBERS):
        back_send[m] = (part_sums[m] + part_logs[m] * incoming).astype(BF16)
    for k in range(1, MEMBERS):
        peer = (me + k) % MEMBERS
        copy = pair(
            back_send.at[peer], back_recv.at[me], sem_b, peer, me, block * MEMBERS + peer
        )
        copy.start()
        sends.append(copy)
    back_recv[me] = back_send[me]
    for k in range(1, MEMBERS):
        peer = (me + k) % MEMBERS
        pair(
            back_send.at[0], back_recv.at[peer], sem_b, me, peer, block * MEMBERS + peer
        ).wait_recv()

    mixed = []
    for s in range(seqs):
        state = back_recv[s * 4 : s * 4 + 4].reshape(64, 128)
        carried = dot(query_s[s], jnp.concatenate([state, state], axis=0))
        gated = (inner_s[s] + carried * cum_s[s]) * gate_s[s]
        mean_sq = jnp.mean(gated * gated, axis=-1, keepdims=True)
        mixed.append(gated * lax.rsqrt(mean_sq + NORM_EPS) * out_gain_ref[...])
    for t in range(8):
        mix_send[t] = jnp.concatenate(
            [part[t * 8 : t * 8 + 8, :] for part in mixed], axis=0
        ).astype(BF16)
    for k in range(1, 8):
        peer = (tp + k) % 8
        copy = remote(
            mix_send.at[peer], mix_recv.at[tp], sem_m.at[0, peer], sem_m.at[1, tp], tp=peer
        )
        copy.start()
        sends.append(copy)
    mix_recv[tp] = mix_send[tp]
    for k in range(1, 8):
        peer = (tp + k) % 8
        remote(
            mix_send.at[0], mix_recv.at[peer], sem_m.at[0, tp], sem_m.at[1, peer], tp=peer
        ).wait_recv()
    rows = jnp.concatenate([mix_recv[t] for t in range(8)], axis=1)
    result = dot(rows, w_out[...])
    out_ref[...] = result.reshape(seqs, 8, result.shape[1]).astype(BF16)

    for copy in gather_sends + sends:
        copy.wait_send()

    @pl.when(sp + 1 < places)
    def _():
        rim(sp + 1).wait_send()

    for k in range(1, blocks):
        @pl.when(block + k < blocks)
        def _():
            for copy in far(k, sp + k * MEMBERS):
                copy.wait_send()


def body(
    tokens, in_gain, gate_weight, input_weight, key_weight, query_weight, step_weight,
    conv_input, conv_key, conv_query, step_bias, decay_rate, decay_extra, out_gain, out_weight,
):
    places = lax.axis_size("sp")
    blocks = places // MEMBERS
    seqs, _, width = tokens.shape
    inner = out_weight.shape[0]
    vmem = pl.BlockSpec(memory_space=pltpu.VMEM)
    smem = pl.BlockSpec(memory_space=pltpu.SMEM)
    anywhere = pl.BlockSpec(memory_space=pl.ANY)
    local = (seqs, 64, 128)
    padded = (seqs, 72, 128)
    dma = pltpu.SemaphoreType.DMA
    return pl.pallas_call(
        functools.partial(mixer_kernel, places, seqs),
        out_shape=jax.ShapeDtypeStruct(tokens.shape, BF16),
        in_specs=[
            anywhere, vmem, anywhere, anywhere, anywhere, anywhere, anywhere,
            vmem, vmem, vmem, smem, smem, vmem, vmem, anywhere,
        ],
        out_specs=vmem,
        scratch_shapes=[
            pltpu.VMEM(tokens.shape, BF16),
            pltpu.VMEM((width, 256), BF16),
            pltpu.VMEM((256, width), BF16),
            pltpu.VMEM((16, width), BF16),
            pltpu.VMEM((inner, width), BF16),
            pltpu.VMEM((8, seqs * 8, width), BF16),
            pltpu.VMEM(local, F32),
            pltpu.VMEM(padded, F32),
            pltpu.VMEM(padded, F32),
            pltpu.VMEM(local, F32),
            pltpu.VMEM(local, F32),
            pltpu.VMEM(local, F32),
            pltpu.VMEM(local, F32),
            pltpu.VMEM(local, F32),
            pltpu.VMEM(local, F32),
            pltpu.VMEM(local, BF16),
            pltpu.VMEM((2, seqs * 8, 128), BF16),
            pltpu.VMEM((2, seqs * 8, 128), BF16),
            pltpu.VMEM((MEMBERS, 16, 128), BF16),
            pltpu.VMEM((MEMBERS, 16, 128), BF16),
            pltpu.VMEM((seqs, 1, 128), F32),
            pltpu.VMEM((MEMBERS, 1, 128), F32),
            pltpu.VMEM((MEMBERS, 16, 128), F32),
            pltpu.VMEM((MEMBERS, 1, 128), F32),
            pltpu.VMEM((16, 128), BF16),
            pltpu.VMEM((1, 128), F32),
            pltpu.VMEM((blocks - 1, 16, 128), BF16),
            pltpu.VMEM((blocks - 1, 1, 128), F32),
            pltpu.VMEM((MEMBERS, 16, 128), BF16),
            pltpu.VMEM((MEMBERS, 16, 128), BF16),
            pltpu.VMEM((8, seqs * 8, 128), BF16),
            pltpu.VMEM((8, seqs * 8, 128), BF16),
            dma((7,)),
            dma((14,)),
            dma((8, 2)),
            dma((2,)),
            dma((2, MEMBERS)),
            dma((2, MEMBERS)),
            dma((2, blocks)),
            dma((2, blocks)),
            dma((2, MEMBERS)),
            dma((2, 8)),
        ],
        compiler_params=pltpu.CompilerParams(collective_id=0, has_side_effects=True),
        name="mixer",
    )(
        tokens, in_gain.reshape(1, width), gate_weight, input_weight, key_weight.T,
        query_weight.T, step_weight.T, conv_input, conv_key, conv_query, step_bias, decay_rate,
        decay_extra, out_gain.reshape(1, 128), out_weight,
    )


def solution(mesh):
    placed = (
        P(None, ("sp", "tp"), None),
        P(),
        P(None, "tp"),
        P(None, "tp"),
        P(None, "tp"),
        P(None, "tp"),
        P(),
        P(None, "tp"),
        P(None, "tp"),
        P(None, "tp"),
        P("tp"),
        P("tp"),
        P(None, "tp", "sp"),
        P("tp"),
        P(),
    )
    return jax.shard_map(
        body, mesh=mesh, in_specs=placed, out_specs=P(None, ("sp", "tp"), None), check_vma=False
    )
```

```python
import functools

import jax
import jax.numpy as jnp
from jax import lax
from jax.experimental import pallas as pl
from jax.experimental.pallas import tpu as pltpu
from jax.sharding import PartitionSpec as P

STATE = 64
NORM_EPS = 1e-06
PRECISE = lax.Precision.HIGHEST
MEMBERS = 16
MESH = pl.DeviceIdType.MESH
F32 = jnp.float32
BF16 = jnp.bfloat16


def rounded(values):
    return values.astype(BF16).astype(F32)


def two_parts(values):
    high = values.astype(BF16)
    return high, (values - high.astype(F32)).astype(BF16)


def three_parts(values):
    high = values.astype(BF16)
    rest = values - high.astype(F32)
    middle = rest.astype(BF16)
    return high, middle, (rest - middle.astype(F32)).astype(BF16)


def silu(values):
    return values / (1.0 + jnp.exp(-values))


def softplus(values):
    return jnp.maximum(values, 0.0) + jnp.log1p(jnp.exp(-jnp.abs(values)))


def dot(a, b, contract=((1,), (0,)), precision=None):
    return lax.dot_general(
        a, b, (contract, ((), ())), precision=precision, preferred_element_type=F32
    )


def mixer_kernel(
    places, seqs,
    tokens_ref, gain_ref, gate_ref, input_ref, key_ref, query_ref, step_ref,
    conv_x_ref, conv_k_ref, conv_q_ref, bias_ref, rate_ref, extra_ref, out_gain_ref, out_w_ref,
    out_ref,
    tok, w_gi, w_kq, w_step, w_out, rows_in,
    gate_s, x_pad, kq_pad, step_s, extra_s,
    xs_s, kq_s, cum_s, inner_s, query_s,
    rim_send, rim_recv,
    chunk_send, chunk_recv, log_send, log_recv, part_sums, part_logs,
    total_send, total_log, total_recv, total_log_recv, back_send, back_recv,
    mix_send, mix_recv,
    sem_load, sem_gs, sem_gr, sem_rim, sem_c, sem_l, sem_t, sem_tl, sem_b, sem_m, sem_known,
):
    blocks = places // MEMBERS
    sp, tp = lax.axis_index("sp"), lax.axis_index("tp")
    block, me = sp // MEMBERS, sp % MEMBERS
    chip, core = tp // 2, tp % 2
    ahead, behind = ((chip + 1) % 4) * 2 + core, ((chip + 3) % 4) * 2 + core
    partner = chip * 2 + 1 - core
    place_y = sp % 4
    row_start = sp - place_y

    def along(chips):
        return (sp + 4 * chips + places) % places

    def tell(stage):
        for chips in (2**stage, -(2**stage)):
            pl.semaphore_signal(
                sem_known.at[stage], inc=1, device_id={"sp": along(chips)}, device_id_type=MESH
            )

    def hear(stage):
        pl.semaphore_wait(sem_known.at[stage], 2)

    def load(k, source, target):
        copy = pltpu.make_async_copy(source, target, sem_load.at[k])
        copy.start()
        return copy

    tok_load = load(0, tokens_ref, tok)
    weight_loads = [
        load(1, gate_ref, w_gi.at[:, 0:128]),
        load(2, input_ref, w_gi.at[:, 128:256]),
        load(3, key_ref, w_kq.at[0:64, :]),
        load(4, query_ref, w_kq.at[64:128, :]),
    ]
    step_load = load(5, step_ref, w_step)
    out_load = load(6, out_w_ref, w_out)

    def remote(source, target, send_sem, recv_sem, **device):
        return pltpu.make_async_remote_copy(
            src_ref=source, dst_ref=target, send_sem=send_sem, recv_sem=recv_sem,
            device_id=device, device_id_type=MESH,
        )

    def pair(source, target, sems, here, there, device):
        return remote(source, target, sems.at[0, here], sems.at[1, there], sp=device)

    for k in range(blocks - 1):
        total_recv[k] = jnp.zeros((16, 128), BF16)
        total_log_recv[k] = jnp.zeros((1, 128), F32)

    @pl.when(sp == 0)
    def _():
        rim_recv[...] = jnp.zeros_like(rim_recv)

    barrier = pltpu.get_barrier_semaphore()

    def greet(**device):
        pl.semaphore_signal(barrier, inc=1, device_id=device, device_id_type=MESH)

    for k in range(1, 8):
        greet(tp=(tp + k) % 8)
    for k in range(1, 4):
        greet(sp=row_start + (place_y + k) % 4)
    greet(sp=along(1))
    greet(sp=along(-1))

    tok_load.wait()
    values = tok[...].astype(F32).reshape(seqs * 8, tok.shape[2])
    mean_sq = jnp.mean(values * values, axis=-1, keepdims=True)
    rows_in[0] = (values * lax.rsqrt(mean_sq + NORM_EPS) * gain_ref[...]).astype(BF16)

    pl.semaphore_wait(barrier, 7 + 3 + 2)

    gather_sends = []

    def pass_on(k, slot, half, to_slot, device):
        part = pl.ds(half * 16, 16)
        copy = remote(
            rows_in.at[slot, part], rows_in.at[to_slot, part],
            sem_gs.at[k], sem_gr.at[to_slot, half], tp=device,
        )
        copy.start()
        gather_sends.append(copy)

    def arrived(slot, half):
        part = pl.ds(half * 16, 16)
        remote(
            rows_in.at[slot, part], rows_in.at[slot, part],
            sem_gs.at[0], sem_gr.at[slot, half], tp=partner,
        ).wait_recv()

    pass_on(0, 0, 0, 4, ahead)
    pass_on(1, 0, 1, 2, behind)
    pass_on(2, 0, 1, 4, ahead)
    pass_on(3, 0, 0, 2, behind)
    pass_on(4, 0, 0, 1, partner)
    pass_on(5, 0, 1, 1, partner)
    tell(0)

    row = lax.broadcasted_iota(jnp.int32, (64, 128), 0)
    lane = lax.broadcasted_iota(jnp.int32, (64, 128), 1)
    inside = lane % 64
    diagonal = row == inside
    causal = row >= inside
    first_head = lane < 64
    lane_row = lax.broadcasted_iota(jnp.int32, (1, 128), 1)
    bias_row = jnp.where(lane_row < 64, bias_ref[0], bias_ref[1])
    rate_row = jnp.where(lane_row < 64, rate_ref[0], rate_ref[1])

    step_load.wait()
    pick_row = lax.broadcasted_iota(jnp.int32, (128, 16), 0) // 64 + 2 * tp
    pick = (pick_row == lax.broadcasted_iota(jnp.int32, (128, 16), 1)).astype(F32).astype(BF16)
    w_kq[128:256, :] = dot(pick, w_step[...]).astype(BF16)
    same_head = (
        lax.broadcasted_iota(jnp.int32, (128, 128), 0) // 64
        == lax.broadcasted_iota(jnp.int32, (128, 128), 1) // 64
    ).astype(F32)
    for s in range(seqs):
        extra_row = jnp.concatenate([extra_ref[s, 0:1, :], extra_ref[s, 1:2, :]], axis=1)
        extra_s[s] = dot(jnp.where(diagonal, extra_row, 0.0), same_head, precision=PRECISE)
    for copy in weight_loads:
        copy.wait()
    hear(0)
    tell(1)

    arrived(4, 0)
    pass_on(6, 4, 0, 6, ahead)
    pass_on(7, 4, 0, 5, partner)
    arrived(2, 1)
    pass_on(8, 2, 1, 6, behind)
    pass_on(9, 2, 1, 3, partner)
    hear(1)
    tell(2)
    arrived(4, 1)
    pass_on(10, 4, 1, 5, partner)
    arrived(2, 0)
    pass_on(11, 2, 0, 3, partner)
    arrived(6, 0)
    pass_on(12, 6, 0, 7, partner)
    arrived(6, 1)
    pass_on(13, 6, 1, 7, partner)
    hear(2)
    tell(3)
    def partner_rows():
        for slot in (1, 3, 5):
            arrived(slot, 0)
            arrived(slot, 1)

    partner_rows()

    position = [
        ((chip + away) % 4) * 2 + (core if same else 1 - core)
        for away in (0, 1, 3, 2)
        for same in (True, False)
    ]

    def project(first, count):
        rows = rows_in[first : first + count].reshape(count * 32, rows_in.shape[2])
        gate_x = rounded(dot(rows, w_gi[...]))
        kq_step = rounded(dot(rows, w_kq[...], ((1,), (1,))))
        for i in range(count):
            at = pl.multiple_of(position[first + i] * 8, 8)
            for s in range(seqs):
                part = slice(i * 32 + s * 8, i * 32 + s * 8 + 8)
                gate_s[s, pl.ds(at, 8), :] = gate_x[part, 0:128]
                x_pad[s, pl.ds(at + 8, 8), :] = gate_x[part, 128:256]
                kq_pad[s, pl.ds(at + 8, 8), :] = kq_step[part, 0:128]
                step_s[s, pl.ds(at, 8), :] = kq_step[part, 128:256]

    project(0, 6)

    def last_rows():
        arrived(7, 0)
        arrived(7, 1)

    last_rows()
    project(6, 2)

    for i, padded in enumerate((x_pad, kq_pad)):
        tails = [padded[s, 64:72, :] for s in range(seqs)]
        rim_send[i] = jnp.concatenate(tails, axis=0).astype(BF16)

    def rim(device):
        return remote(rim_send, rim_recv, sem_rim.at[0], sem_rim.at[1], sp=device)

    @pl.when(sp + 1 < places)
    def _():
        rim(sp + 1).start()

    triangle = (
        lax.broadcasted_iota(jnp.int32, (64, 192), 0)
        >= lax.broadcasted_iota(jnp.int32, (64, 192), 1) % 64
    ).astype(F32).astype(BF16)
    for s in range(seqs):
        step = softplus(step_s[s] + bias_row)
        step_s[s] = step
        log_decay = extra_s[s] - step * rate_row
        cum = dot(triangle, jnp.concatenate(three_parts(log_decay), axis=0))
        cum_s[s] = cum
        log_send[s] = cum[63:64, :]

    def rim_rows():
        @pl.when(sp > 0)
        def _():
            rim(sp - 1).wait_recv()

    rim_rows()

    conv_kq = jnp.concatenate([conv_k_ref[...], conv_q_ref[...]], axis=1)
    rim_x, rim_kq = rim_recv[0].astype(F32), rim_recv[1].astype(F32)
    for s in range(seqs):
        x_pad[s, 0:8, :] = rim_x[s * 8 : s * 8 + 8, :]
        kq_pad[s, 0:8, :] = rim_kq[s * 8 : s * 8 + 8, :]
        x_sum = x_pad[s, 5:69, :] * conv_x_ref[0:1, :]
        kq_sum = kq_pad[s, 5:69, :] * conv_kq[0:1, :]
        for k in range(1, 4):
            x_sum = x_sum + x_pad[s, 5 + k : 69 + k, :] * conv_x_ref[k : k + 1, :]
            kq_sum = kq_sum + kq_pad[s, 5 + k : 69 + k, :] * conv_kq[k : k + 1, :]
        scaled = silu(x_sum) * step_s[s]
        kq = silu(kq_sum)
        xs_s[s] = scaled
        kq_s[s] = kq
        cum = cum_s[s]
        x_high, x_low = two_parts(scaled * jnp.exp(cum[63:64, :] - cum))
        k_high, k_low = two_parts(kq[:, 0:64])
        state = dot(
            jnp.concatenate([k_high, k_high, k_low], axis=0),
            jnp.concatenate([x_high, x_low, x_high], axis=0),
            ((0,), (0,)),
        )
        for q in range(4):
            chunk_send[s * 4 + q] = state[q * 16 : q * 16 + 16, :].astype(BF16)

    sends = []
    for k in range(1, MEMBERS):
        peer = (me + k) % MEMBERS
        device = block * MEMBERS + peer
        one = pair(log_send.at[peer // 4], log_recv.at[me], sem_l, peer, me, device)
        one.start()
        two = pair(chunk_send.at[peer], chunk_recv.at[me], sem_c, peer, me, device)
        two.start()
        sends += [one, two]
    chunk_recv[me] = chunk_send[me]
    log_recv[me] = log_send[me // 4]

    for s in range(seqs):
        cum, kq, scaled = cum_s[s], kq_s[s], xs_s[s]
        keys, queries = kq[:, 0:64], kq[:, 64:128]
        query_s[s] = jnp.concatenate(two_parts(queries), axis=1)
        cum_row = jnp.sum(jnp.where(diagonal, cum, 0.0), axis=0, keepdims=True)
        decay = jnp.where(causal, jnp.exp(jnp.where(causal, cum - cum_row, 0.0)), 0.0)
        scores = dot(queries, jnp.concatenate([keys, keys], axis=0), ((1,), (1,)), PRECISE)
        apart = jnp.concatenate(
            [jnp.where(first_head, scaled, 0.0), jnp.where(first_head, 0.0, scaled)], axis=0
        )
        inner_s[s] = dot(scores * decay, apart, precision=PRECISE)
        cum_s[s] = jnp.exp(cum)
        gate_s[s] = silu(gate_s[s])

    def chunks_here():
        for k in range(1, MEMBERS):
            peer = (me + k) % MEMBERS
            device = block * MEMBERS + peer
            pair(log_send.at[0], log_recv.at[peer], sem_l, me, peer, device).wait_recv()
            pair(chunk_send.at[0], chunk_recv.at[peer], sem_c, me, peer, device).wait_recv()

    chunks_here()

    running = jnp.zeros((16, 128), F32)
    log_sum = jnp.zeros((1, 128), F32)
    for m in range(MEMBERS):
        part_sums[m] = running
        part_logs[m] = log_sum
        here = log_recv[m]
        running = jnp.exp(here) * running + chunk_recv[m].astype(F32)
        log_sum = log_sum + here
    total_send[...] = running.astype(BF16)
    total_log[...] = log_sum

    hear(3)

    def far(k, device):
        return (
            pair(total_log, total_log_recv.at[k - 1], sem_tl, k - 1, k - 1, device),
            pair(total_send, total_recv.at[k - 1], sem_t, k - 1, k - 1, device),
        )

    for k in range(1, blocks):
        @pl.when(block + k < blocks)
        def _():
            for copy in far(k, sp + k * MEMBERS):
                copy.start()
    for m in range(MEMBERS):
        part_logs[m] = jnp.exp(part_logs[m])
    out_load.wait()

    def totals_here():
        for k in range(1, blocks):
            @pl.when(block >= k)
            def _():
                for copy in far(k, sp - k * MEMBERS):
                    copy.wait_recv()

    totals_here()
    incoming = jnp.zeros((16, 128), F32)
    for k in range(blocks - 1, 0, -1):
        incoming = jnp.exp(total_log_recv[k - 1]) * incoming + total_recv[k - 1].astype(F32)
    for m in range(MEMBERS):
        back_send[m] = (part_sums[m] + part_logs[m] * incoming).astype(BF16)
    for k in range(1, MEMBERS):
        peer = (me + k) % MEMBERS
        copy = pair(
            back_send.at[peer], back_recv.at[me], sem_b, peer, me, block * MEMBERS + peer
        )
        copy.start()
        sends.append(copy)
    back_recv[me] = back_send[me]

    def states_here():
        for k in range(1, MEMBERS):
            peer = (me + k) % MEMBERS
            pair(
                back_send.at[0], back_recv.at[peer], sem_b, me, peer, block * MEMBERS + peer
            ).wait_recv()

    states_here()

    mixed = []
    for s in range(seqs):
        state = back_recv[s * 4 : s * 4 + 4].reshape(64, 128)
        carried = dot(query_s[s], jnp.concatenate([state, state], axis=0))
        gated = (inner_s[s] + carried * cum_s[s]) * gate_s[s]
        mean_sq = jnp.mean(gated * gated, axis=-1, keepdims=True)
        mixed.append(gated * lax.rsqrt(mean_sq + NORM_EPS) * out_gain_ref[...])
    for t in range(8):
        mix_send[t] = jnp.concatenate(
            [part[t * 8 : t * 8 + 8, :] for part in mixed], axis=0
        ).astype(BF16)
    for k in range(1, 8):
        peer = (tp + k) % 8
        copy = remote(
            mix_send.at[peer], mix_recv.at[tp], sem_m.at[0, peer], sem_m.at[1, tp], tp=peer
        )
        copy.start()
        sends.append(copy)
    mix_recv[tp] = mix_send[tp]

    def heads_here():
        for k in range(1, 8):
            peer = (tp + k) % 8
            remote(
                mix_send.at[0], mix_recv.at[peer], sem_m.at[0, tp], sem_m.at[1, peer], tp=peer
            ).wait_recv()

    heads_here()
    rows = jnp.concatenate([mix_recv[t] for t in range(8)], axis=1)
    result = dot(rows, w_out[...])
    out_ref[...] = result.reshape(seqs, 8, result.shape[1]).astype(BF16)

    for copy in gather_sends + sends:
        copy.wait_send()

    @pl.when(sp + 1 < places)
    def _():
        rim(sp + 1).wait_send()

    for k in range(1, blocks):
        @pl.when(block + k < blocks)
        def _():
            for copy in far(k, sp + k * MEMBERS):
                copy.wait_send()


def body(
    tokens, in_gain, gate_weight, input_weight, key_weight, query_weight, step_weight,
    conv_input, conv_key, conv_query, step_bias, decay_rate, decay_extra, out_gain, out_weight,
):
    places = lax.axis_size("sp")
    blocks = places // MEMBERS
    seqs, _, width = tokens.shape
    inner = out_weight.shape[0]
    vmem = pl.BlockSpec(memory_space=pltpu.VMEM)
    smem = pl.BlockSpec(memory_space=pltpu.SMEM)
    anywhere = pl.BlockSpec(memory_space=pl.ANY)
    local = (seqs, 64, 128)
    padded = (seqs, 72, 128)
    dma = pltpu.SemaphoreType.DMA
    return pl.pallas_call(
        functools.partial(mixer_kernel, places, seqs),
        out_shape=jax.ShapeDtypeStruct(tokens.shape, BF16),
        in_specs=[
            anywhere, vmem, anywhere, anywhere, anywhere, anywhere, anywhere,
            vmem, vmem, vmem, smem, smem, vmem, vmem, anywhere,
        ],
        out_specs=vmem,
        scratch_shapes=[
            pltpu.VMEM(tokens.shape, BF16),
            pltpu.VMEM((width, 256), BF16),
            pltpu.VMEM((256, width), BF16),
            pltpu.VMEM((16, width), BF16),
            pltpu.VMEM((inner, width), BF16),
            pltpu.VMEM((8, seqs * 8, width), BF16),
            pltpu.VMEM(local, F32),
            pltpu.VMEM(padded, F32),
            pltpu.VMEM(padded, F32),
            pltpu.VMEM(local, F32),
            pltpu.VMEM(local, F32),
            pltpu.VMEM(local, F32),
            pltpu.VMEM(local, F32),
            pltpu.VMEM(local, F32),
            pltpu.VMEM(local, F32),
            pltpu.VMEM(local, BF16),
            pltpu.VMEM((2, seqs * 8, 128), BF16),
            pltpu.VMEM((2, seqs * 8, 128), BF16),
            pltpu.VMEM((MEMBERS, 16, 128), BF16),
            pltpu.VMEM((MEMBERS, 16, 128), BF16),
            pltpu.VMEM((seqs, 1, 128), F32),
            pltpu.VMEM((MEMBERS, 1, 128), F32),
            pltpu.VMEM((MEMBERS, 16, 128), F32),
            pltpu.VMEM((MEMBERS, 1, 128), F32),
            pltpu.VMEM((16, 128), BF16),
            pltpu.VMEM((1, 128), F32),
            pltpu.VMEM((blocks - 1, 16, 128), BF16),
            pltpu.VMEM((blocks - 1, 1, 128), F32),
            pltpu.VMEM((MEMBERS, 16, 128), BF16),
            pltpu.VMEM((MEMBERS, 16, 128), BF16),
            pltpu.VMEM((8, seqs * 8, 128), BF16),
            pltpu.VMEM((8, seqs * 8, 128), BF16),
            dma((7,)),
            dma((14,)),
            dma((8, 2)),
            dma((2,)),
            dma((2, MEMBERS)),
            dma((2, MEMBERS)),
            dma((2, blocks)),
            dma((2, blocks)),
            dma((2, MEMBERS)),
            dma((2, 8)),
            pltpu.SemaphoreType.REGULAR((4,)),
        ],
        compiler_params=pltpu.CompilerParams(collective_id=0, has_side_effects=True),
        name="mixer",
    )(
        tokens, in_gain.reshape(1, width), gate_weight, input_weight, key_weight.T,
        query_weight.T, step_weight.T, conv_input, conv_key, conv_query, step_bias, decay_rate,
        decay_extra, out_gain.reshape(1, 128), out_weight,
    )


def solution(mesh):
    placed = (
        P(None, ("sp", "tp"), None),
        P(),
        P(None, "tp"),
        P(None, "tp"),
        P(None, "tp"),
        P(None, "tp"),
        P(),
        P(None, "tp"),
        P(None, "tp"),
        P(None, "tp"),
        P("tp"),
        P("tp"),
        P(None, "tp", "sp"),
        P("tp"),
        P(),
    )
    return jax.shard_map(
        body, mesh=mesh, in_specs=placed, out_specs=P(None, ("sp", "tp"), None), check_vma=False
    )
```

```python
import functools

import jax
import jax.numpy as jnp
from jax import lax
from jax.experimental import pallas as pl
from jax.experimental.pallas import tpu as pltpu
from jax.sharding import PartitionSpec as P

STATE = 64
NORM_EPS = 1e-06
PRECISE = lax.Precision.HIGHEST
MEMBERS = 16
MESH = pl.DeviceIdType.MESH
F32 = jnp.float32
BF16 = jnp.bfloat16


def rounded(values):
    return values.astype(BF16).astype(F32)


def two_parts(values):
    high = values.astype(BF16)
    return high, (values - high.astype(F32)).astype(BF16)


def three_parts(values):
    high = values.astype(BF16)
    rest = values - high.astype(F32)
    middle = rest.astype(BF16)
    return high, middle, (rest - middle.astype(F32)).astype(BF16)


def silu(values):
    return values / (1.0 + jnp.exp(-values))


def softplus(values):
    return jnp.maximum(values, 0.0) + jnp.log1p(jnp.exp(-jnp.abs(values)))


def dot(a, b, contract=((1,), (0,)), precision=None):
    return lax.dot_general(
        a, b, (contract, ((), ())), precision=precision, preferred_element_type=F32
    )


def mixer_kernel(
    places, seqs,
    tokens_ref, gain_ref, gate_ref, input_ref, key_ref, query_ref, step_ref,
    conv_x_ref, conv_k_ref, conv_q_ref, bias_ref, rate_ref, extra_ref, out_gain_ref,
    out_ref,
    tok, gain, w_gi, w_kq, w_step, conv_x, conv_k, conv_q, bias, rate, extra, out_gain,
    rows_in, tail_out, tail_in,
    gate_s, x_pad, kq_pad, step_s, extra_s,
    xs_s, kq_s, cum_s, inner_s, query_s,
    chunk_send, chunk_recv, log_send, log_recv, part_sums, part_logs,
    total_send, total_log, total_recv, total_log_recv, back_send, back_recv,
    mix_send,
    sem_load, sem_gs, sem_gr, sem_tail, sem_c, sem_l, sem_t, sem_tl, sem_b, sem_m, sem_known,
):
    blocks = places // MEMBERS
    sp, tp = lax.axis_index("sp"), lax.axis_index("tp")
    block, me = sp // MEMBERS, sp % MEMBERS
    chip, core = tp // 2, tp % 2
    ahead, behind = ((chip + 1) % 4) * 2 + core, ((chip + 3) % 4) * 2 + core
    partner = chip * 2 + 1 - core
    place_y = sp % 4
    row_start = sp - place_y

    def along(chips):
        return (sp + 4 * chips + places) % places

    stages = ((1, -1, 2, -2), (4, -4), (8, -8))

    def tell(stage):
        for chips in stages[stage]:
            pl.semaphore_signal(
                sem_known.at[stage], inc=1, device_id={"sp": along(chips)}, device_id_type=MESH
            )

    def hear(stage):
        pl.semaphore_wait(sem_known.at[stage], len(stages[stage]))
        pl.semaphore_signal(
            sem_known.at[stage], inc=1, device_id={"tp": partner}, device_id_type=MESH
        )
        if stage + 1 < len(stages):
            tell(stage + 1)

    def relay(stage):
        @pl.when(core == 1)
        def _():
            hear(stage)

    def learn(stage):
        @pl.when(core == 0)
        def _():
            pl.semaphore_wait(sem_known.at[stage], 1)

    def load(k, source, target):
        copy = pltpu.make_async_copy(source, target, sem_load.at[k])
        copy.start()
        return copy

    tok_load = load(0, tokens_ref, tok)

    def remote(source, target, send_sem, recv_sem, **device):
        return pltpu.make_async_remote_copy(
            src_ref=source, dst_ref=target, send_sem=send_sem, recv_sem=recv_sem,
            device_id=device, device_id_type=MESH,
        )

    def pair(source, target, sems, device):
        return remote(source, target, sems.at[0], sems.at[1], sp=device)

    def all_done(buffer, sem):
        pltpu.make_async_copy(buffer, buffer, sem).wait()

    for k in range(blocks - 1):
        total_recv[k] = jnp.zeros((16, 128), BF16)
        total_log_recv[k] = jnp.zeros((1, 128), F32)

    @pl.when(sp == 0)
    def _():
        tail_in[...] = jnp.zeros_like(tail_in)

    barrier = pltpu.get_barrier_semaphore()

    def greet(**device):
        pl.semaphore_signal(barrier, inc=1, device_id=device, device_id_type=MESH)

    for k in range(1, 8):
        greet(tp=(tp + k) % 8)
    for k in range(1, 4):
        greet(sp=row_start + (place_y + k) % 4, tp=chip * 2 + 1)
    for chips in stages[0]:
        greet(sp=along(chips), tp=chip * 2 + 1)

    from_tail = (core == 1) & (chip != 1)

    @pl.when((sp > 0) & from_tail)
    def _():
        greet(sp=sp - 1, tp=7)

    weight_loads = [
        load(1, gain_ref, gain),
        load(2, step_ref, w_step),
        load(3, extra_ref, extra),
        load(4, gate_ref, w_gi.at[:, 0:128]),
        load(4, input_ref, w_gi.at[:, 128:256]),
        load(5, key_ref, w_kq.at[0:64, :]),
        load(5, query_ref, w_kq.at[64:128, :]),
        load(6, conv_x_ref, conv_x),
        load(7, conv_k_ref, conv_k),
        load(8, conv_q_ref, conv_q),
        load(9, bias_ref, bias),
        load(10, rate_ref, rate),
        load(11, out_gain_ref, out_gain),
    ]
    gain_load, step_load, extra_load = weight_loads[0:3]
    weight_loads = weight_loads[7:]

    tok_load.wait()
    gain_load.wait()
    values = tok[...].astype(F32)
    mean_sq = jnp.mean(values * values, axis=-1, keepdims=True)
    normed = values * lax.rsqrt(mean_sq + NORM_EPS) * gain[...]
    rows_in[0] = normed.reshape(seqs * 8, tok.shape[2]).astype(BF16)

    has_tail = (tp == 7) & (sp + 1 < places)

    @pl.when(has_tail)
    def _():
        tail_out[...] = normed[:, 4:8, :].reshape(seqs * 4, tok.shape[2]).astype(BF16)

    def entry():
        @pl.when(core == 0)
        def _():
            pl.semaphore_wait(barrier, 7)

        @pl.when((core == 1) & ~has_tail)
        def _():
            pl.semaphore_wait(barrier, 7 + 6 + 8)

        @pl.when(has_tail)
        def _():
            pl.semaphore_wait(barrier, 7 + 6 + 8 + 3)

    entry()

    width = tok.shape[2]

    def quarter(slot, part):
        columns = pl.ds(part % 2 * (width // 2), width // 2)
        return rows_in.at[slot, pl.ds(part // 2 * 16, 16), columns]

    def landing(slot, part):
        if slot in (4, 5, 6):
            return sem_gr.at[(slot - 4) * 4 + part]
        return sem_gr.at[12 if slot < 4 else 13]

    def pass_on(slot, part, to_slot, device):
        remote(
            quarter(slot, part), quarter(to_slot, part),
            sem_gs.at[0], landing(to_slot, part), tp=device,
        ).start()

    def arrived(slot, *parts):
        for part in parts:
            all_done(quarter(slot, part), landing(slot, part))

    for part in range(4):
        pass_on(0, part, 5, ahead)
        pass_on(0, (part + 2) % 4, 4, behind)
    for part in range(4):
        pass_on(0, part, 1, partner)

    def tail(k, source, **device):
        return remote(source, tail_in, sem_tail.at[k], sem_tail.at[5], **device)

    @pl.when(has_tail)
    def _():
        for k, target in enumerate((7, 1, 5)):
            tail(k, tail_out, sp=sp + 1, tp=target).start()

    @pl.when(core == 1)
    def _():
        tell(0)

    row = lax.broadcasted_iota(jnp.int32, (64, 128), 0)
    lane = lax.broadcasted_iota(jnp.int32, (64, 128), 1)
    inside = lane % 64
    diagonal = row == inside
    causal = row >= inside
    first_head = lane < 64
    lane_row = lax.broadcasted_iota(jnp.int32, (1, 128), 1)

    step_load.wait()
    extra_load.wait()
    pick_row = lax.broadcasted_iota(jnp.int32, (128, 16), 0) // 64 + 2 * tp
    pick = (pick_row == lax.broadcasted_iota(jnp.int32, (128, 16), 1)).astype(F32).astype(BF16)
    w_kq[128:256, :] = dot(pick, w_step[...]).astype(BF16)
    same_head = (
        lax.broadcasted_iota(jnp.int32, (128, 128), 0) // 64
        == lax.broadcasted_iota(jnp.int32, (128, 128), 1) // 64
    ).astype(F32)
    for s in range(seqs):
        extra_row = jnp.concatenate([extra[s, 0:1, :], extra[s, 1:2, :]], axis=1)
        extra_s[s] = dot(jnp.where(diagonal, extra_row, 0.0), same_head, precision=PRECISE)
    all_done(w_gi, sem_load.at[4])
    all_done(w_kq.at[pl.ds(0, 128)], sem_load.at[5])
    for copy in weight_loads:
        copy.wait()
    bias_row = jnp.where(lane_row < 64, bias[:, 0:1], bias[:, 1:2])
    rate_row = jnp.where(lane_row < 64, rate[:, 0:1], rate[:, 1:2])
    relay(0)

    arrived(5, 0)
    pass_on(5, 0, 6, ahead)
    arrived(4, 2)
    pass_on(4, 2, 6, behind)
    arrived(5, 1)
    pass_on(5, 1, 6, ahead)
    arrived(4, 3)
    pass_on(4, 3, 6, behind)
    for part in (0, 1):
        pass_on(5, part, 3, partner)
        pass_on(4, part + 2, 2, partner)

    def tail_first():
        @pl.when((sp > 0) & from_tail)
        def _():
            tail(0, tail_out, tp=partner).wait_recv()
            tail(4, tail_in, tp=partner).start()

            @pl.when(chip == 0)
            def _():
                tail(3, tail_in, tp=ahead).start()

    for part in (2, 3):
        arrived(5, part)
        pass_on(5, part, 3, partner)
    for part in (0, 1):
        arrived(4, part)
        pass_on(4, part, 2, partner)
    tail_first()
    def opposite_rows():
        for part in range(4):
            arrived(6, part)
            pass_on(6, part, 7, partner)

    def partner_rows():
        all_done(rows_in.at[pl.ds(1, 3)], sem_gr.at[12])

    position = [
        ((chip + away) % 4) * 2 + (core if same else 1 - core)
        for away, same in (
            (0, True), (0, False), (1, False), (3, False),
            (1, True), (3, True), (2, True), (2, False),
        )
    ]

    def project(first, count, more=()):
        rows = rows_in[first : first + count].reshape(count * 32, width)
        rows = jnp.concatenate([rows, *more], axis=0)
        gate_x = rounded(dot(rows, w_gi[...]))
        kq_step = rounded(dot(rows, w_kq[...], ((1,), (1,))))
        for i in range(count):
            at = pl.multiple_of(position[first + i] * 8, 8)
            for s in range(seqs):
                part = slice(i * 32 + s * 8, i * 32 + s * 8 + 8)
                gate_s[s, pl.ds(at, 8), :] = gate_x[part, 0:128]
                x_pad[s, pl.ds(at + 8, 8), :] = gate_x[part, 128:256]
                kq_pad[s, pl.ds(at + 8, 8), :] = kq_step[part, 0:128]
                step_s[s, pl.ds(at, 8), :] = kq_step[part, 128:256]
        if more:
            for s in range(seqs):
                part = slice(count * 32 + s * 4 + 1, count * 32 + s * 4 + 4)
                x_pad[s, 5:8, :] = gate_x[part, 128:256]
                kq_pad[s, 5:8, :] = kq_step[part, 0:128]

    def tail_last():
        @pl.when((sp > 0) & (core == 1) & (chip == 1))
        def _():
            tail(0, tail_out, tp=partner).wait_recv()
            tail(4, tail_in, tp=partner).start()

        @pl.when((sp > 0) & (core == 0))
        def _():
            tail(0, tail_out, tp=partner).wait_recv()

    relay(1)

    @pl.when(core == 1)
    def _():
        opposite_rows()

    partner_rows()
    project(0, 6)

    @pl.when(core == 0)
    def _():
        opposite_rows()

    def last_rows():
        all_done(rows_in.at[7], sem_gr.at[13])

    last_rows()
    tail_last()
    project(6, 2, (tail_in[...],))
    triangle = (
        lax.broadcasted_iota(jnp.int32, (64, 192), 0)
        >= lax.broadcasted_iota(jnp.int32, (64, 192), 1) % 64
    ).astype(F32).astype(BF16)
    for s in range(seqs):
        step = softplus(step_s[s] + bias_row)
        step_s[s] = step
        log_decay = extra_s[s] - step * rate_row
        cum = dot(triangle, jnp.concatenate(three_parts(log_decay), axis=0))
        cum_s[s] = cum
        log_send[s] = cum[63:64, :]

    def members():
        for k in range(1, MEMBERS):
            peer = (me + k) % MEMBERS
            yield peer, block * MEMBERS + peer

    learn(0)
    learn(1)
    for peer, device in members():
        copy = pair(log_send.at[peer // 4], log_recv.at[me], sem_l, device)
        copy.start()
    log_recv[me] = log_send[me // 4]

    conv_kq = jnp.concatenate([conv_k[...], conv_q[...]], axis=1)
    for s in range(seqs):
        x_sum = x_pad[s, 5:69, :] * conv_x[0:1, :]
        kq_sum = kq_pad[s, 5:69, :] * conv_kq[0:1, :]
        for k in range(1, 4):
            x_sum = x_sum + x_pad[s, 5 + k : 69 + k, :] * conv_x[k : k + 1, :]
            kq_sum = kq_sum + kq_pad[s, 5 + k : 69 + k, :] * conv_kq[k : k + 1, :]
        scaled = silu(x_sum) * step_s[s]
        kq = silu(kq_sum)
        xs_s[s] = scaled
        kq_s[s] = kq
        cum = cum_s[s]
        x_high, x_low = two_parts(scaled * jnp.exp(cum[63:64, :] - cum))
        k_high, k_low = two_parts(kq[:, 0:64])
        state = dot(
            jnp.concatenate([k_high, k_high, k_low], axis=0),
            jnp.concatenate([x_high, x_low, x_high], axis=0),
            ((0,), (0,)),
        )
        for q in range(4):
            chunk_send[s * 4 + q] = state[q * 16 : q * 16 + 16, :].astype(BF16)

    for peer, device in members():
        copy = pair(chunk_send.at[peer], chunk_recv.at[me], sem_c, device)
        copy.start()
    chunk_recv[me] = chunk_send[me]

    for s in range(seqs):
        cum, kq, scaled = cum_s[s], kq_s[s], xs_s[s]
        keys, queries = kq[:, 0:64], kq[:, 64:128]
        query_s[s] = jnp.concatenate(two_parts(queries), axis=1)
        cum_row = jnp.sum(jnp.where(diagonal, cum, 0.0), axis=0, keepdims=True)
        decay = jnp.where(causal, jnp.exp(jnp.where(causal, cum - cum_row, 0.0)), 0.0)
        scores = dot(queries, jnp.concatenate([keys, keys], axis=0), ((1,), (1,)), PRECISE)
        apart = jnp.concatenate(
            [jnp.where(first_head, scaled, 0.0), jnp.where(first_head, 0.0, scaled)], axis=0
        )
        inner_s[s] = dot(scores * decay, apart, precision=PRECISE)
        cum_s[s] = jnp.exp(cum)
        gate_s[s] = silu(gate_s[s])

    def logs_here():
        all_done(log_recv.at[pl.ds(0, MEMBERS - 1)], sem_l.at[1])

    def chunks_here():
        all_done(chunk_recv.at[pl.ds(0, MEMBERS - 1)], sem_c.at[1])

    def far_log(k, device):
        return pair(total_log, total_log_recv.at[k - 1], sem_tl, device)

    def far(k, device):
        return pair(total_send, total_recv.at[k - 1], sem_t, device)

    def later_blocks(act):
        for k in range(1, blocks):
            @pl.when(block + k < blocks)
            def _():
                act(k, sp + k * MEMBERS)

    def count_done(count, side):
        for k in range(1, blocks):
            @pl.when(count == k)
            def _():
                all_done(total_log_recv.at[pl.ds(0, k)], sem_tl.at[side])
                all_done(total_recv.at[pl.ds(0, k)], sem_t.at[side])

    def rows_sent():
        all_done(rows_in.at[pl.ds(0, 7)], sem_gs.at[0])

        @pl.when(has_tail)
        def _():
            for k in range(3):
                tail(k, tail_out, sp=sp + 1, tp=7).wait_send()

        @pl.when((sp > 0) & (core == 1))
        def _():
            tail(4, tail_in, tp=partner).wait_send()

            @pl.when(chip == 0)
            def _():
                tail(3, tail_in, tp=ahead).wait_send()

    rows_sent()

    logs_here()
    log_sum = jnp.zeros((1, 128), F32)
    for m in range(MEMBERS):
        part_logs[m] = jnp.exp(log_sum)
        log_sum = log_sum + log_recv[m]
        log_recv[m] = jnp.exp(log_recv[m])
    total_log[...] = log_sum
    chunks_here()
    running = jnp.zeros((16, 128), F32)
    for m in range(MEMBERS):
        part_sums[m] = running
        running = log_recv[m] * running + chunk_recv[m].astype(F32)
    total_send[...] = running.astype(BF16)
    relay(2)
    learn(2)
    later_blocks(lambda k, device: far_log(k, device).start())
    later_blocks(lambda k, device: far(k, device).start())

    def totals_here():
        count_done(block, 1)

    totals_here()
    incoming = jnp.zeros((16, 128), F32)
    for k in range(blocks - 1, 0, -1):
        incoming = jnp.exp(total_log_recv[k - 1]) * incoming + total_recv[k - 1].astype(F32)
    for m in range(MEMBERS):
        back_send[m] = (part_sums[m] + part_logs[m] * incoming).astype(BF16)
    for peer, device in members():
        copy = pair(back_send.at[peer], back_recv.at[me], sem_b, device)
        copy.start()
    back_recv[me] = back_send[me]

    def parts_sent():
        all_done(log_recv.at[pl.ds(0, MEMBERS - 1)], sem_l.at[0])
        all_done(chunk_recv.at[pl.ds(0, MEMBERS - 1)], sem_c.at[0])
        all_done(back_recv.at[pl.ds(0, MEMBERS - 1)], sem_b.at[0])
        count_done(blocks - 1 - block, 0)

    parts_sent()

    def states_here():
        all_done(back_recv.at[pl.ds(0, MEMBERS - 1)], sem_b.at[1])

    states_here()

    mixed = []
    for s in range(seqs):
        state = back_recv[s * 4 : s * 4 + 4].reshape(64, 128)
        carried = dot(query_s[s], jnp.concatenate([state, state], axis=0))
        gated = (inner_s[s] + carried * cum_s[s]) * gate_s[s]
        mean_sq = jnp.mean(gated * gated, axis=-1, keepdims=True)
        mixed.append(gated * lax.rsqrt(mean_sq + NORM_EPS) * out_gain[...])
    for t in range(8):
        mix_send[t] = jnp.concatenate(
            [part[t * 8 : t * 8 + 8, :] for part in mixed], axis=0
        ).astype(BF16)

    def columns(source):
        return out_ref.at[:, pl.ds(pl.multiple_of(source * 128, 128), 128)]

    for k in range(1, 8):
        peer = (tp + k) % 8
        copy = remote(
            mix_send.at[peer], columns(tp), sem_m.at[0], sem_m.at[1], tp=peer
        )
        copy.start()
    own = pltpu.make_async_copy(mix_send.at[tp], columns(tp), sem_m.at[2])
    own.start()

    def heads_here():
        all_done(mix_send.at[pl.ds(0, 7)], sem_m.at[1])

    heads_here()
    def heads_sent():
        own.wait()
        all_done(mix_send.at[pl.ds(0, 7)], sem_m.at[0])

    heads_sent()


def body(
    tokens, in_gain, gate_weight, input_weight, key_weight, query_weight, step_weight,
    conv_input, conv_key, conv_query, step_bias, decay_rate, decay_extra, out_gain, out_weight,
):
    places = lax.axis_size("sp")
    blocks = places // MEMBERS
    seqs, _, width = tokens.shape
    inner = out_weight.shape[0]
    local = (seqs, 64, 128)
    padded = (seqs, 72, 128)
    dma = pltpu.SemaphoreType.DMA
    vmem = pltpu.VMEM
    operands = (
        tokens, in_gain.reshape(1, width), gate_weight, input_weight, key_weight.T,
        query_weight.T, step_weight.T, conv_input, conv_key, conv_query,
        step_bias.reshape(1, 2), decay_rate.reshape(1, 2), decay_extra,
        out_gain.reshape(1, 128),
    )
    rows = pl.pallas_call(
        functools.partial(mixer_kernel, places, seqs),
        out_shape=jax.ShapeDtypeStruct((seqs * 8, inner), BF16),
        in_specs=[pl.BlockSpec(memory_space=pl.ANY)] * 14,
        out_specs=pl.BlockSpec(memory_space=pl.ANY),
        scratch_shapes=[
            vmem(tokens.shape, BF16),
            vmem((1, width), F32),
            vmem((width, 256), BF16),
            vmem((256, width), BF16),
            vmem((16, width), BF16),
            vmem(conv_input.shape, F32),
            vmem(conv_key.shape, F32),
            vmem(conv_query.shape, F32),
            vmem((1, 2), F32),
            vmem((1, 2), F32),
            vmem(decay_extra.shape, F32),
            vmem((1, 128), F32),
            vmem((8, seqs * 8, width), BF16),
            vmem((seqs * 4, width), BF16),
            vmem((seqs * 4, width), BF16),
            vmem(local, F32),
            vmem(padded, F32),
            vmem(padded, F32),
            vmem(local, F32),
            vmem(local, F32),
            vmem(local, F32),
            vmem(local, F32),
            vmem(local, F32),
            vmem(local, F32),
            vmem(local, BF16),
            vmem((MEMBERS, 16, 128), BF16),
            vmem((MEMBERS, 16, 128), BF16),
            vmem((seqs, 1, 128), F32),
            vmem((MEMBERS, 1, 128), F32),
            vmem((MEMBERS, 16, 128), F32),
            vmem((MEMBERS, 1, 128), F32),
            vmem((16, 128), BF16),
            vmem((1, 128), F32),
            vmem((blocks - 1, 16, 128), BF16),
            vmem((blocks - 1, 1, 128), F32),
            vmem((MEMBERS, 16, 128), BF16),
            vmem((MEMBERS, 16, 128), BF16),
            vmem((8, seqs * 8, 128), BF16),
            dma((12,)),
            dma((1,)),
            dma((14,)),
            dma((6,)),
            dma((2,)),
            dma((2,)),
            dma((2,)),
            dma((2,)),
            dma((2,)),
            dma((3,)),
            pltpu.SemaphoreType.REGULAR((3,)),
        ],
        compiler_params=pltpu.CompilerParams(
            collective_id=0, has_side_effects=True, vmem_limit_bytes=16 * 2**20
        ),
        cost_estimate=pl.CostEstimate(
            flops=4 * 10**9, bytes_accessed=2 * 2**20, transcendentals=0
        ),
        name="mixer",
    )(*[pltpu.with_memory_space_constraint(operand, pltpu.HBM) for operand in operands])
    result = jnp.dot(rows, out_weight, preferred_element_type=F32)
    return result.astype(BF16).reshape(tokens.shape)


def solution(mesh):
    placed = (
        P(None, ("sp", "tp"), None),
        P(),
        P(None, "tp"),
        P(None, "tp"),
        P(None, "tp"),
        P(None, "tp"),
        P(),
        P(None, "tp"),
        P(None, "tp"),
        P(None, "tp"),
        P("tp"),
        P("tp"),
        P(None, "tp", "sp"),
        P("tp"),
        P(),
    )
    return jax.shard_map(
        body, mesh=mesh, in_specs=placed, out_specs=P(None, ("sp", "tp"), None), check_vma=False
    )
```

```python
import functools

import jax
import jax.numpy as jnp
from jax import lax
from jax.experimental import pallas as pl
from jax.experimental.pallas import tpu as pltpu
from jax.sharding import PartitionSpec as P

STATE = 64
NORM_EPS = 1e-06
PRECISE = lax.Precision.HIGHEST
MEMBERS = 16
MESH = pl.DeviceIdType.MESH
F32 = jnp.float32
BF16 = jnp.bfloat16


def rounded(values):
    return values.astype(BF16).astype(F32)


def two_parts(values):
    high = values.astype(BF16)
    return high, (values - high.astype(F32)).astype(BF16)


def three_parts(values):
    high = values.astype(BF16)
    rest = values - high.astype(F32)
    middle = rest.astype(BF16)
    return high, middle, (rest - middle.astype(F32)).astype(BF16)


def silu(values):
    return values / (1.0 + jnp.exp(-values))


def softplus(values):
    return jnp.maximum(values, 0.0) + jnp.log1p(jnp.exp(-jnp.abs(values)))


def dot(a, b, contract=((1,), (0,)), precision=None):
    return lax.dot_general(
        a, b, (contract, ((), ())), precision=precision, preferred_element_type=F32
    )


def mixer_kernel(
    places, seqs,
    tokens_ref, gain_ref, gate_ref, input_ref, key_ref, query_ref, step_ref,
    conv_x_ref, conv_k_ref, conv_q_ref, bias_ref, rate_ref, extra_ref, out_gain_ref,
    out_ref,
    tok, gain, w_gi, w_kq, w_step, conv_x, conv_k, conv_q, bias, rate, extra, out_gain,
    rows_in, tail_out, tail_in,
    gate_s, x_pad, kq_pad, step_s, extra_s,
    xs_s, kq_s, cum_s, inner_s, query_s,
    chunk_send, chunk_recv, log_send, log_recv, part_sums, part_logs,
    total_send, total_log, total_recv, total_log_recv, back_send, back_recv,
    mix_send,
    sem_load, sem_gs, sem_gr, sem_tail, sem_c, sem_l, sem_t, sem_tl, sem_b, sem_m, sem_known,
):
    blocks = places // MEMBERS
    sp, tp = lax.axis_index("sp"), lax.axis_index("tp")
    block, me = sp // MEMBERS, sp % MEMBERS
    chip, core = tp // 2, tp % 2
    ahead, behind = ((chip + 1) % 4) * 2 + core, ((chip + 3) % 4) * 2 + core
    partner = chip * 2 + 1 - core
    place_y = sp % 4
    row_start = sp - place_y

    def along(chips):
        return (sp + 4 * chips + places) % places

    stages = ((1, -1, 2, -2), (4, -4), (8, -8))

    def tell(stage):
        for chips in stages[stage]:
            pl.semaphore_signal(
                sem_known.at[stage], inc=1, device_id={"sp": along(chips)}, device_id_type=MESH
            )

    def hear(stage):
        pl.semaphore_wait(sem_known.at[stage], len(stages[stage]))
        pl.semaphore_signal(
            sem_known.at[stage], inc=1, device_id={"tp": partner}, device_id_type=MESH
        )
        if stage + 1 < len(stages):
            tell(stage + 1)

    def relay(stage):
        @pl.when(core == 1)
        def _():
            hear(stage)

    def learn(stage):
        @pl.when(core == 0)
        def _():
            pl.semaphore_wait(sem_known.at[stage], 1)

    def load(k, source, target):
        copy = pltpu.make_async_copy(source, target, sem_load.at[k])
        copy.start()
        return copy

    tok_load = load(0, tokens_ref, tok)

    def remote(source, target, send_sem, recv_sem, **device):
        return pltpu.make_async_remote_copy(
            src_ref=source, dst_ref=target, send_sem=send_sem, recv_sem=recv_sem,
            device_id=device, device_id_type=MESH,
        )

    def pair(source, target, sems, device):
        return remote(source, target, sems.at[0], sems.at[1], sp=device)

    def all_done(buffer, sem):
        pltpu.make_async_copy(buffer, buffer, sem).wait()

    for k in range(blocks - 1):
        total_recv[k] = jnp.zeros((16, 128), BF16)
        total_log_recv[k] = jnp.zeros((1, 128), F32)

    @pl.when(sp == 0)
    def _():
        tail_in[...] = jnp.zeros_like(tail_in)

    barrier = pltpu.get_barrier_semaphore()

    def greet(**device):
        pl.semaphore_signal(barrier, inc=1, device_id=device, device_id_type=MESH)

    for k in range(1, 8):
        greet(tp=(tp + k) % 8)
    for k in range(1, 4):
        greet(sp=row_start + (place_y + k) % 4, tp=chip * 2 + 1)
    for chips in stages[0]:
        greet(sp=along(chips), tp=chip * 2 + 1)

    from_tail = (core == 1) & (chip != 1)

    @pl.when((sp > 0) & from_tail)
    def _():
        greet(sp=sp - 1, tp=7)

    weight_loads = [
        load(1, gain_ref, gain),
        load(2, step_ref, w_step),
        load(3, extra_ref, extra),
        load(4, gate_ref, w_gi.at[:, 0:128]),
        load(4, input_ref, w_gi.at[:, 128:256]),
        load(5, key_ref, w_kq.at[0:64, :]),
        load(5, query_ref, w_kq.at[64:128, :]),
        load(6, conv_x_ref, conv_x),
        load(7, conv_k_ref, conv_k),
        load(8, conv_q_ref, conv_q),
        load(9, bias_ref, bias),
        load(10, rate_ref, rate),
        load(11, out_gain_ref, out_gain),
    ]
    gain_load, step_load, extra_load = weight_loads[0:3]
    weight_loads = weight_loads[7:]

    tok_load.wait()
    gain_load.wait()
    values = tok[...].astype(F32)
    mean_sq = jnp.mean(values * values, axis=-1, keepdims=True)
    normed = values * lax.rsqrt(mean_sq + NORM_EPS) * gain[...]
    rows_in[0] = normed.reshape(seqs * 8, tok.shape[2]).astype(BF16)

    has_tail = (tp == 7) & (sp + 1 < places)

    @pl.when(has_tail)
    def _():
        tail_out[...] = normed[:, 4:8, :].reshape(seqs * 4, tok.shape[2]).astype(BF16)

    def entry():
        @pl.when(core == 0)
        def _():
            pl.semaphore_wait(barrier, 7)
            pl.semaphore_signal(
                sem_known.at[3], inc=1, device_id={"tp": partner}, device_id_type=MESH
            )

        @pl.when(core == 1)
        def _():
            pl.semaphore_wait(sem_known.at[3], 1)

    def entry_near():
        @pl.when((core == 1) & ~has_tail)
        def _():
            pl.semaphore_wait(barrier, 7 + 6 + 8)

        @pl.when(has_tail)
        def _():
            pl.semaphore_wait(barrier, 7 + 6 + 8 + 3)

    entry()

    width = tok.shape[2]

    def quarter(slot, part):
        columns = pl.ds(part % 2 * (width // 2), width // 2)
        return rows_in.at[slot, pl.ds(part // 2 * 16, 16), columns]

    def landing(slot, part):
        if slot in (4, 5, 6):
            return sem_gr.at[(slot - 4) * 4 + part]
        return sem_gr.at[12 if slot < 4 else 13]

    def pass_on(slot, part, to_slot, device):
        remote(
            quarter(slot, part), quarter(to_slot, part),
            sem_gs.at[0], landing(to_slot, part), tp=device,
        ).start()

    def arrived(slot, *parts):
        for part in parts:
            all_done(quarter(slot, part), landing(slot, part))

    for part in range(4):
        pass_on(0, part, 5, ahead)
        pass_on(0, (part + 2) % 4, 4, behind)
    for part in range(4):
        pass_on(0, part, 1, partner)

    def tail(k, source, **device):
        return remote(source, tail_in, sem_tail.at[k], sem_tail.at[5], **device)

    row = lax.broadcasted_iota(jnp.int32, (64, 128), 0)
    lane = lax.broadcasted_iota(jnp.int32, (64, 128), 1)
    inside = lane % 64
    diagonal = row == inside
    causal = row >= inside
    first_head = lane < 64
    lane_row = lax.broadcasted_iota(jnp.int32, (1, 128), 1)

    step_load.wait()
    extra_load.wait()
    pick_row = lax.broadcasted_iota(jnp.int32, (128, 16), 0) // 64 + 2 * tp
    pick = (pick_row == lax.broadcasted_iota(jnp.int32, (128, 16), 1)).astype(F32).astype(BF16)
    w_kq[128:256, :] = dot(pick, w_step[...]).astype(BF16)
    same_head = (
        lax.broadcasted_iota(jnp.int32, (128, 128), 0) // 64
        == lax.broadcasted_iota(jnp.int32, (128, 128), 1) // 64
    ).astype(F32)
    for s in range(seqs):
        extra_row = jnp.concatenate([extra[s, 0:1, :], extra[s, 1:2, :]], axis=1)
        extra_s[s] = dot(jnp.where(diagonal, extra_row, 0.0), same_head, precision=PRECISE)
    entry_near()

    @pl.when(has_tail)
    def _():
        for k, target in enumerate((7, 1, 5)):
            tail(k, tail_out, sp=sp + 1, tp=target).start()

    @pl.when(core == 1)
    def _():
        tell(0)

    all_done(w_gi, sem_load.at[4])
    all_done(w_kq.at[pl.ds(0, 128)], sem_load.at[5])
    for copy in weight_loads:
        copy.wait()
    bias_row = jnp.where(lane_row < 64, bias[:, 0:1], bias[:, 1:2])
    rate_row = jnp.where(lane_row < 64, rate[:, 0:1], rate[:, 1:2])
    arrived(5, 0)
    pass_on(5, 0, 6, ahead)
    arrived(4, 2)
    pass_on(4, 2, 6, behind)
    arrived(5, 1)
    pass_on(5, 1, 6, ahead)
    arrived(4, 3)
    pass_on(4, 3, 6, behind)
    for part in (0, 1):
        pass_on(5, part, 3, partner)
        pass_on(4, part + 2, 2, partner)
    def tail_first():
        @pl.when((sp > 0) & from_tail)
        def _():
            tail(0, tail_out, tp=partner).wait_recv()
            tail(4, tail_in, tp=partner).start()

            @pl.when(chip == 0)
            def _():
                tail(3, tail_in, tp=ahead).start()

    for part in (2, 3):
        arrived(5, part)
        pass_on(5, part, 3, partner)
    for part in (0, 1):
        arrived(4, part)
        pass_on(4, part, 2, partner)
    relay(0)
    tail_first()
    def opposite_rows():
        for part in range(4):
            arrived(6, part)
            pass_on(6, part, 7, partner)

    def partner_rows():
        all_done(rows_in.at[pl.ds(1, 3)], sem_gr.at[12])

    position = [
        ((chip + away) % 4) * 2 + (core if same else 1 - core)
        for away, same in (
            (0, True), (0, False), (1, False), (3, False),
            (1, True), (3, True), (2, True), (2, False),
        )
    ]

    def project(first, count, more=()):
        rows = rows_in[first : first + count].reshape(count * 32, width)
        rows = jnp.concatenate([rows, *more], axis=0)
        gate_x = rounded(dot(rows, w_gi[...]))
        kq_step = rounded(dot(rows, w_kq[...], ((1,), (1,))))
        for i in range(count):
            at = pl.multiple_of(position[first + i] * 8, 8)
            for s in range(seqs):
                part = slice(i * 32 + s * 8, i * 32 + s * 8 + 8)
                gate_s[s, pl.ds(at, 8), :] = gate_x[part, 0:128]
                x_pad[s, pl.ds(at + 8, 8), :] = gate_x[part, 128:256]
                kq_pad[s, pl.ds(at + 8, 8), :] = kq_step[part, 0:128]
                step_s[s, pl.ds(at, 8), :] = kq_step[part, 128:256]
        if more:
            for s in range(seqs):
                part = slice(count * 32 + s * 4 + 1, count * 32 + s * 4 + 4)
                x_pad[s, 5:8, :] = gate_x[part, 128:256]
                kq_pad[s, 5:8, :] = kq_step[part, 0:128]

    def tail_last():
        @pl.when((sp > 0) & (core == 1) & (chip == 1))
        def _():
            tail(0, tail_out, tp=partner).wait_recv()
            tail(4, tail_in, tp=partner).start()

        @pl.when((sp > 0) & (core == 0))
        def _():
            tail(0, tail_out, tp=partner).wait_recv()

    @pl.when(core == 1)
    def _():
        opposite_rows()


    partner_rows()
    project(0, 6)

    @pl.when(core == 0)
    def _():
        opposite_rows()

    def last_rows():
        all_done(rows_in.at[7], sem_gr.at[13])

    last_rows()
    tail_last()
    project(6, 2, (tail_in[...],))
    triangle = (
        lax.broadcasted_iota(jnp.int32, (64, 192), 0)
        >= lax.broadcasted_iota(jnp.int32, (64, 192), 1) % 64
    ).astype(F32).astype(BF16)
    for s in range(seqs):
        step = softplus(step_s[s] + bias_row)
        step_s[s] = step
        log_decay = extra_s[s] - step * rate_row
        cum = dot(triangle, jnp.concatenate(three_parts(log_decay), axis=0))
        cum_s[s] = cum
        log_send[s] = cum[63:64, :]

    def members():
        for chips in (3, 1, 2, 0):
            for k in (2, 1, 3, 0):
                if chips or k:
                    peer = (me // 4 + chips) % 4 * 4 + (me + k) % 4
                    yield peer, block * MEMBERS + peer

    relay(1)
    learn(0)
    learn(1)
    for peer, device in members():
        copy = pair(log_send.at[peer // 4], log_recv.at[me], sem_l, device)
        copy.start()
    log_recv[me] = log_send[me // 4]

    conv_kq = jnp.concatenate([conv_k[...], conv_q[...]], axis=1)
    for s in range(seqs):
        x_sum = x_pad[s, 5:69, :] * conv_x[0:1, :]
        kq_sum = kq_pad[s, 5:69, :] * conv_kq[0:1, :]
        for k in range(1, 4):
            x_sum = x_sum + x_pad[s, 5 + k : 69 + k, :] * conv_x[k : k + 1, :]
            kq_sum = kq_sum + kq_pad[s, 5 + k : 69 + k, :] * conv_kq[k : k + 1, :]
        scaled = silu(x_sum) * step_s[s]
        kq = silu(kq_sum)
        xs_s[s] = scaled
        kq_s[s] = kq
        cum = cum_s[s]
        x_high, x_low = two_parts(scaled * jnp.exp(cum[63:64, :] - cum))
        k_high, k_low = two_parts(kq[:, 0:64])
        state = dot(
            jnp.concatenate([k_high, k_high, k_low], axis=0),
            jnp.concatenate([x_high, x_low, x_high], axis=0),
            ((0,), (0,)),
        )
        for q in range(4):
            chunk_send[s * 4 + q] = state[q * 16 : q * 16 + 16, :].astype(BF16)

    for peer, device in members():
        copy = pair(chunk_send.at[peer], chunk_recv.at[me], sem_c, device)
        copy.start()
    chunk_recv[me] = chunk_send[me]

    for s in range(seqs):
        cum, kq, scaled = cum_s[s], kq_s[s], xs_s[s]
        keys, queries = kq[:, 0:64], kq[:, 64:128]
        query_s[s] = jnp.concatenate(two_parts(queries), axis=1)
        cum_row = jnp.sum(jnp.where(diagonal, cum, 0.0), axis=0, keepdims=True)
        decay = jnp.where(causal, jnp.exp(jnp.where(causal, cum - cum_row, 0.0)), 0.0)
        scores = dot(queries, jnp.concatenate([keys, keys], axis=0), ((1,), (1,)), PRECISE)
        apart = jnp.concatenate(
            [jnp.where(first_head, scaled, 0.0), jnp.where(first_head, 0.0, scaled)], axis=0
        )
        inner_s[s] = dot(scores * decay, apart, precision=PRECISE)
        cum_s[s] = jnp.exp(cum)
        gate_s[s] = silu(gate_s[s])

    def logs_here():
        all_done(log_recv.at[pl.ds(0, MEMBERS - 1)], sem_l.at[1])

    def chunks_here():
        all_done(chunk_recv.at[pl.ds(0, MEMBERS - 1)], sem_c.at[1])

    def far_log(k, device):
        return pair(total_log, total_log_recv.at[k - 1], sem_tl, device)

    def far(k, device):
        return pair(total_send, total_recv.at[k - 1], sem_t, device)

    def later_blocks(act):
        for k in sorted(range(1, blocks), key=lambda k: abs(2 * k - blocks)):
            @pl.when(block + k < blocks)
            def _():
                act(k, sp + k * MEMBERS)

    def count_done(count, side):
        for k in range(1, blocks):
            @pl.when(count == k)
            def _():
                all_done(total_log_recv.at[pl.ds(0, k)], sem_tl.at[side])
                all_done(total_recv.at[pl.ds(0, k)], sem_t.at[side])

    def rows_sent():
        all_done(rows_in.at[pl.ds(0, 7)], sem_gs.at[0])

        @pl.when(has_tail)
        def _():
            for k in range(3):
                tail(k, tail_out, sp=sp + 1, tp=7).wait_send()

        @pl.when((sp > 0) & (core == 1))
        def _():
            tail(4, tail_in, tp=partner).wait_send()

            @pl.when(chip == 0)
            def _():
                tail(3, tail_in, tp=ahead).wait_send()

    rows_sent()

    logs_here()
    log_sum = jnp.zeros((1, 128), F32)
    for m in range(MEMBERS):
        part_logs[m] = jnp.exp(log_sum)
        log_sum = log_sum + log_recv[m]
        log_recv[m] = jnp.exp(log_recv[m])
    total_log[...] = log_sum
    chunks_here()
    running = jnp.zeros((16, 128), F32)
    for m in range(MEMBERS):
        part_sums[m] = running
        running = log_recv[m] * running + chunk_recv[m].astype(F32)
    total_send[...] = running.astype(BF16)
    relay(2)
    learn(2)

    def send_far(k, device):
        far_log(k, device).start()
        far(k, device).start()

    later_blocks(send_far)

    def totals_here():
        count_done(block, 1)

    totals_here()
    incoming = jnp.zeros((16, 128), F32)
    for k in range(blocks - 1, 0, -1):
        incoming = jnp.exp(total_log_recv[k - 1]) * incoming + total_recv[k - 1].astype(F32)
    for m in range(MEMBERS):
        back_send[m] = (part_sums[m] + part_logs[m] * incoming).astype(BF16)
    for peer, device in members():
        copy = pair(back_send.at[peer], back_recv.at[me], sem_b, device)
        copy.start()
    back_recv[me] = back_send[me]

    def parts_sent():
        all_done(log_recv.at[pl.ds(0, MEMBERS - 1)], sem_l.at[0])
        all_done(chunk_recv.at[pl.ds(0, MEMBERS - 1)], sem_c.at[0])
        all_done(back_recv.at[pl.ds(0, MEMBERS - 1)], sem_b.at[0])
        count_done(blocks - 1 - block, 0)

    parts_sent()

    def states_here():
        all_done(back_recv.at[pl.ds(0, MEMBERS - 1)], sem_b.at[1])

    states_here()

    mixed = []
    for s in range(seqs):
        state = back_recv[s * 4 : s * 4 + 4].reshape(64, 128)
        carried = dot(query_s[s], jnp.concatenate([state, state], axis=0))
        gated = (inner_s[s] + carried * cum_s[s]) * gate_s[s]
        mean_sq = jnp.mean(gated * gated, axis=-1, keepdims=True)
        mixed.append(gated * lax.rsqrt(mean_sq + NORM_EPS) * out_gain[...])
    for t in range(8):
        mix_send[t] = jnp.concatenate(
            [part[t * 8 : t * 8 + 8, :] for part in mixed], axis=0
        ).astype(BF16)

    def columns(source):
        return out_ref.at[:, pl.ds(pl.multiple_of(source * 128, 128), 128)]

    for chips in (2, 1, 3, 0):
        for same in (True, False):
            if chips or not same:
                peer = (chip + chips) % 4 * 2 + (core if same else 1 - core)
                remote(
                    mix_send.at[peer], columns(tp), sem_m.at[0], sem_m.at[1], tp=peer
                ).start()
    own = pltpu.make_async_copy(mix_send.at[tp], columns(tp), sem_m.at[2])
    own.start()

    def heads_here():
        all_done(mix_send.at[pl.ds(0, 7)], sem_m.at[1])

    heads_here()
    def heads_sent():
        own.wait()
        all_done(mix_send.at[pl.ds(0, 7)], sem_m.at[0])

    heads_sent()


def body(
    tokens, in_gain, gate_weight, input_weight, key_weight, query_weight, step_weight,
    conv_input, conv_key, conv_query, step_bias, decay_rate, decay_extra, out_gain, out_weight,
):
    places = lax.axis_size("sp")
    blocks = places // MEMBERS
    seqs, _, width = tokens.shape
    inner = out_weight.shape[0]
    local = (seqs, 64, 128)
    padded = (seqs, 72, 128)
    dma = pltpu.SemaphoreType.DMA
    vmem = pltpu.VMEM
    operands = (
        tokens, in_gain.reshape(1, width), gate_weight, input_weight, key_weight.T,
        query_weight.T, step_weight.T, conv_input, conv_key, conv_query,
        step_bias.reshape(1, 2), decay_rate.reshape(1, 2), decay_extra,
        out_gain.reshape(1, 128),
    )
    rows = pl.pallas_call(
        functools.partial(mixer_kernel, places, seqs),
        out_shape=jax.ShapeDtypeStruct((seqs * 8, inner), BF16),
        in_specs=[pl.BlockSpec(memory_space=pl.ANY)] * 14,
        out_specs=pl.BlockSpec(memory_space=pl.ANY),
        scratch_shapes=[
            vmem(tokens.shape, BF16),
            vmem((1, width), F32),
            vmem((width, 256), BF16),
            vmem((256, width), BF16),
            vmem((16, width), BF16),
            vmem(conv_input.shape, F32),
            vmem(conv_key.shape, F32),
            vmem(conv_query.shape, F32),
            vmem((1, 2), F32),
            vmem((1, 2), F32),
            vmem(decay_extra.shape, F32),
            vmem((1, 128), F32),
            vmem((8, seqs * 8, width), BF16),
            vmem((seqs * 4, width), BF16),
            vmem((seqs * 4, width), BF16),
            vmem(local, F32),
            vmem(padded, F32),
            vmem(padded, F32),
            vmem(local, F32),
            vmem(local, F32),
            vmem(local, F32),
            vmem(local, F32),
            vmem(local, F32),
            vmem(local, F32),
            vmem(local, BF16),
            vmem((MEMBERS, 16, 128), BF16),
            vmem((MEMBERS, 16, 128), BF16),
            vmem((seqs, 1, 128), F32),
            vmem((MEMBERS, 1, 128), F32),
            vmem((MEMBERS, 16, 128), F32),
            vmem((MEMBERS, 1, 128), F32),
            vmem((16, 128), BF16),
            vmem((1, 128), F32),
            vmem((blocks - 1, 16, 128), BF16),
            vmem((blocks - 1, 1, 128), F32),
            vmem((MEMBERS, 16, 128), BF16),
            vmem((MEMBERS, 16, 128), BF16),
            vmem((8, seqs * 8, 128), BF16),
            dma((12,)),
            dma((1,)),
            dma((14,)),
            dma((6,)),
            dma((2,)),
            dma((2,)),
            dma((2,)),
            dma((2,)),
            dma((2,)),
            dma((3,)),
            pltpu.SemaphoreType.REGULAR((4,)),
        ],
        compiler_params=pltpu.CompilerParams(
            collective_id=0, has_side_effects=True, vmem_limit_bytes=16 * 2**20
        ),
        cost_estimate=pl.CostEstimate(
            flops=4 * 10**9, bytes_accessed=2 * 2**20, transcendentals=0
        ),
        name="mixer",
    )(*[pltpu.with_memory_space_constraint(operand, pltpu.HBM) for operand in operands])
    result = jnp.dot(rows, out_weight, preferred_element_type=F32)
    return result.astype(BF16).reshape(tokens.shape)


def solution(mesh):
    placed = (
        P(None, ("sp", "tp"), None),
        P(),
        P(None, "tp"),
        P(None, "tp"),
        P(None, "tp"),
        P(None, "tp"),
        P(),
        P(None, "tp"),
        P(None, "tp"),
        P(None, "tp"),
        P("tp"),
        P("tp"),
        P(None, "tp", "sp"),
        P("tp"),
        P(),
    )
    return jax.shard_map(
        body, mesh=mesh, in_specs=placed, out_specs=P(None, ("sp", "tp"), None), check_vma=False
    )
```

```python
import functools

import jax
import jax.numpy as jnp
from jax import lax
from jax.experimental import pallas as pl
from jax.experimental.pallas import tpu as pltpu
from jax.sharding import PartitionSpec as P

STATE = 64
NORM_EPS = 1e-06
PRECISE = lax.Precision.HIGHEST
MEMBERS = 16
MESH = pl.DeviceIdType.MESH
F32 = jnp.float32
BF16 = jnp.bfloat16


def rounded(values):
    return values.astype(BF16).astype(F32)


def two_parts(values):
    high = values.astype(BF16)
    return high, (values - high.astype(F32)).astype(BF16)


def three_parts(values):
    high = values.astype(BF16)
    rest = values - high.astype(F32)
    middle = rest.astype(BF16)
    return high, middle, (rest - middle.astype(F32)).astype(BF16)


def silu(values):
    return values / (1.0 + jnp.exp(-values))


def softplus(values):
    return jnp.maximum(values, 0.0) + jnp.log1p(jnp.exp(-jnp.abs(values)))


def dot(a, b, contract=((1,), (0,)), precision=None):
    return lax.dot_general(
        a, b, (contract, ((), ())), precision=precision, preferred_element_type=F32
    )


def mixer_kernel(
    places, seqs,
    tokens_ref, gain_ref, gate_ref, input_ref, key_ref, query_ref, step_ref,
    conv_x_ref, conv_k_ref, conv_q_ref, bias_ref, rate_ref, extra_ref, out_gain_ref,
    out_ref,
    tok, gain, w_gi, w_kq, w_step, conv_x, conv_k, conv_q, bias, rate, extra, out_gain,
    rows_in, tail_out, tail_in,
    gate_s, x_pad, kq_pad, step_s, extra_s,
    xs_s, kq_s, cum_s, inner_s, query_s,
    chunk_send, chunk_recv, log_send, log_recv, part_sums, part_logs,
    total_send, total_log, total_recv, total_log_recv, back_send, back_recv,
    mix_send,
    sem_load, sem_gs, sem_gr, sem_tail, sem_c, sem_l, sem_t, sem_tl, sem_b, sem_m, sem_known,
):
    blocks = places // MEMBERS
    sp, tp = lax.axis_index("sp"), lax.axis_index("tp")
    block, me = sp // MEMBERS, sp % MEMBERS
    chip, core = tp // 2, tp % 2
    ahead, behind = ((chip + 1) % 4) * 2 + core, ((chip + 3) % 4) * 2 + core
    partner = chip * 2 + 1 - core
    place_y = sp % 4
    row_start = sp - place_y

    def along(chips):
        return (sp + 4 * chips + places) % places

    stages = ((1, -1, 2, -2), (4, -4), (8, -8))

    def tell(stage):
        for chips in stages[stage]:
            pl.semaphore_signal(
                sem_known.at[stage], inc=1, device_id={"sp": along(chips)}, device_id_type=MESH
            )

    def hear(stage):
        pl.semaphore_wait(sem_known.at[stage], len(stages[stage]))
        pl.semaphore_signal(
            sem_known.at[stage], inc=1, device_id={"tp": partner}, device_id_type=MESH
        )
        if stage + 1 < len(stages):
            tell(stage + 1)

    def relay(stage):
        @pl.when(core == 1)
        def _():
            hear(stage)

    def learn(stage):
        @pl.when(core == 0)
        def _():
            pl.semaphore_wait(sem_known.at[stage], 1)

    def load(k, source, target):
        copy = pltpu.make_async_copy(source, target, sem_load.at[k])
        copy.start()
        return copy

    tok_load = load(0, tokens_ref, tok)

    def remote(source, target, send_sem, recv_sem, **device):
        return pltpu.make_async_remote_copy(
            src_ref=source, dst_ref=target, send_sem=send_sem, recv_sem=recv_sem,
            device_id=device, device_id_type=MESH,
        )

    def pair(source, target, sems, device):
        return remote(source, target, sems.at[0], sems.at[1], sp=device)

    def all_done(buffer, sem):
        pltpu.make_async_copy(buffer, buffer, sem).wait()

    for k in range(blocks - 1):
        total_recv[k] = jnp.zeros((16, 128), BF16)
        total_log_recv[k] = jnp.zeros((1, 128), F32)

    @pl.when(sp == 0)
    def _():
        tail_in[...] = jnp.zeros_like(tail_in)

    barrier = pltpu.get_barrier_semaphore()

    def greet(**device):
        pl.semaphore_signal(barrier, inc=1, device_id=device, device_id_type=MESH)

    for k in range(1, 8):
        greet(tp=(tp + k) % 8)
    for k in range(1, 4):
        greet(sp=row_start + (place_y + k) % 4, tp=chip * 2 + 1)
    for chips in stages[0]:
        greet(sp=along(chips), tp=chip * 2 + 1)

    from_tail = (core == 1) & (chip != 1)

    @pl.when((sp > 0) & from_tail)
    def _():
        greet(sp=sp - 1, tp=7)

    weight_loads = [
        load(1, gain_ref, gain),
        load(2, step_ref, w_step),
        load(3, extra_ref, extra),
        load(4, gate_ref, w_gi.at[:, 0:128]),
        load(4, input_ref, w_gi.at[:, 128:256]),
        load(5, key_ref, w_kq.at[0:64, :]),
        load(5, query_ref, w_kq.at[64:128, :]),
        load(6, conv_x_ref, conv_x),
        load(7, conv_k_ref, conv_k),
        load(8, conv_q_ref, conv_q),
        load(9, bias_ref, bias),
        load(10, rate_ref, rate),
        load(11, out_gain_ref, out_gain),
    ]
    gain_load, step_load, extra_load = weight_loads[0:3]
    weight_loads = weight_loads[7:]

    tok_load.wait()
    gain_load.wait()
    values = tok[...].astype(F32)
    mean_sq = jnp.mean(values * values, axis=-1, keepdims=True)
    normed = values * lax.rsqrt(mean_sq + NORM_EPS) * gain[...]
    rows_in[0] = normed.reshape(seqs * 8, tok.shape[2]).astype(BF16)

    has_tail = (tp == 7) & (sp + 1 < places)

    @pl.when(has_tail)
    def _():
        tail_out[...] = normed[:, 4:8, :].reshape(seqs * 4, tok.shape[2]).astype(BF16)

    def entry():
        @pl.when(core == 0)
        def _():
            pl.semaphore_wait(barrier, 7)
            pl.semaphore_signal(
                sem_known.at[3], inc=1, device_id={"tp": partner}, device_id_type=MESH
            )

        @pl.when(core == 1)
        def _():
            pl.semaphore_wait(sem_known.at[3], 1)

    def entry_near():
        @pl.when((core == 1) & ~has_tail)
        def _():
            pl.semaphore_wait(barrier, 7 + 6 + 8)

        @pl.when(has_tail)
        def _():
            pl.semaphore_wait(barrier, 7 + 6 + 8 + 3)

    entry()

    width = tok.shape[2]

    def quarter(slot, part):
        columns = pl.ds(part % 2 * (width // 2), width // 2)
        return rows_in.at[slot, pl.ds(part // 2 * 16, 16), columns]

    def landing(slot, part):
        if slot in (4, 5, 6):
            return sem_gr.at[(slot - 4) * 4 + part]
        return sem_gr.at[12 if slot < 4 else 13]

    def pass_on(slot, part, to_slot, device):
        remote(
            quarter(slot, part), quarter(to_slot, part),
            sem_gs.at[0], landing(to_slot, part), tp=device,
        ).start()

    def arrived(slot, *parts):
        for part in parts:
            all_done(quarter(slot, part), landing(slot, part))

    for part in range(4):
        pass_on(0, part, 5, ahead)
        pass_on(0, (part + 2) % 4, 4, behind)
    for part in range(4):
        pass_on(0, part, 1, partner)

    def tail(k, source, **device):
        return remote(source, tail_in, sem_tail.at[k], sem_tail.at[5], **device)

    entry_near()

    @pl.when(has_tail)
    def _():
        for k, target in enumerate((7, 1, 5)):
            tail(k, tail_out, sp=sp + 1, tp=target).start()

    @pl.when(core == 1)
    def _():
        tell(0)

    row = lax.broadcasted_iota(jnp.int32, (64, 128), 0)
    lane = lax.broadcasted_iota(jnp.int32, (64, 128), 1)
    inside = lane % 64
    diagonal = row == inside
    causal = row >= inside
    first_head = lane < 64
    lane_row = lax.broadcasted_iota(jnp.int32, (1, 128), 1)

    step_load.wait()
    extra_load.wait()
    pick_row = lax.broadcasted_iota(jnp.int32, (128, 16), 0) // 64 + 2 * tp
    pick = (pick_row == lax.broadcasted_iota(jnp.int32, (128, 16), 1)).astype(F32).astype(BF16)
    w_kq[128:256, :] = dot(pick, w_step[...]).astype(BF16)
    same_head = (
        lax.broadcasted_iota(jnp.int32, (128, 128), 0) // 64
        == lax.broadcasted_iota(jnp.int32, (128, 128), 1) // 64
    ).astype(F32)
    for s in range(seqs):
        extra_row = jnp.concatenate([extra[s, 0:1, :], extra[s, 1:2, :]], axis=1)
        extra_s[s] = dot(jnp.where(diagonal, extra_row, 0.0), same_head, precision=PRECISE)
    all_done(w_gi, sem_load.at[4])
    all_done(w_kq.at[pl.ds(0, 128)], sem_load.at[5])
    for copy in weight_loads:
        copy.wait()
    bias_row = jnp.where(lane_row < 64, bias[:, 0:1], bias[:, 1:2])
    rate_row = jnp.where(lane_row < 64, rate[:, 0:1], rate[:, 1:2])
    relay(0)

    arrived(5, 0)
    pass_on(5, 0, 6, ahead)
    arrived(4, 2)
    pass_on(4, 2, 6, behind)
    arrived(5, 1)
    pass_on(5, 1, 6, ahead)
    arrived(4, 3)
    pass_on(4, 3, 6, behind)
    for part in (0, 1):
        pass_on(5, part, 3, partner)
        pass_on(4, part + 2, 2, partner)
    def tail_first():
        @pl.when((sp > 0) & from_tail)
        def _():
            tail(0, tail_out, tp=partner).wait_recv()
            tail(4, tail_in, tp=partner).start()

            @pl.when(chip == 0)
            def _():
                tail(3, tail_in, tp=ahead).start()

    for part in (2, 3):
        arrived(5, part)
        pass_on(5, part, 3, partner)
    for part in (0, 1):
        arrived(4, part)
        pass_on(4, part, 2, partner)
    tail_first()
    def opposite_rows():
        for part in range(4):
            arrived(6, part)
            pass_on(6, part, 7, partner)

    def partner_rows():
        all_done(rows_in.at[pl.ds(1, 3)], sem_gr.at[12])

    position = [
        ((chip + away) % 4) * 2 + (core if same else 1 - core)
        for away, same in (
            (0, True), (0, False), (1, False), (3, False),
            (1, True), (3, True), (2, True), (2, False),
        )
    ]

    def project(first, count, more=()):
        rows = rows_in[first : first + count].reshape(count * 32, width)
        rows = jnp.concatenate([rows, *more], axis=0)
        gate_x = rounded(dot(rows, w_gi[...]))
        kq_step = rounded(dot(rows, w_kq[...], ((1,), (1,))))
        for i in range(count):
            at = pl.multiple_of(position[first + i] * 8, 8)
            for s in range(seqs):
                part = slice(i * 32 + s * 8, i * 32 + s * 8 + 8)
                gate_s[s, pl.ds(at, 8), :] = gate_x[part, 0:128]
                x_pad[s, pl.ds(at + 8, 8), :] = gate_x[part, 128:256]
                kq_pad[s, pl.ds(at + 8, 8), :] = kq_step[part, 0:128]
                step_s[s, pl.ds(at, 8), :] = kq_step[part, 128:256]
        if more:
            for s in range(seqs):
                part = slice(count * 32 + s * 4 + 1, count * 32 + s * 4 + 4)
                x_pad[s, 5:8, :] = gate_x[part, 128:256]
                kq_pad[s, 5:8, :] = kq_step[part, 0:128]

    def tail_last():
        @pl.when((sp > 0) & (core == 1) & (chip == 1))
        def _():
            tail(0, tail_out, tp=partner).wait_recv()
            tail(4, tail_in, tp=partner).start()

        @pl.when((sp > 0) & (core == 0))
        def _():
            tail(0, tail_out, tp=partner).wait_recv()

    relay(1)

    @pl.when(core == 1)
    def _():
        opposite_rows()


    partner_rows()
    project(0, 6)

    @pl.when(core == 0)
    def _():
        opposite_rows()

    def last_rows():
        all_done(rows_in.at[7], sem_gr.at[13])

    last_rows()
    tail_last()
    project(6, 2, (tail_in[...],))
    triangle = (
        lax.broadcasted_iota(jnp.int32, (64, 192), 0)
        >= lax.broadcasted_iota(jnp.int32, (64, 192), 1) % 64
    ).astype(F32).astype(BF16)
    for s in range(seqs):
        step = softplus(step_s[s] + bias_row)
        step_s[s] = step
        log_decay = extra_s[s] - step * rate_row
        cum = dot(triangle, jnp.concatenate(three_parts(log_decay), axis=0))
        cum_s[s] = cum
        log_send[s] = cum[63:64, :]

    def members():
        for chips in (3, 1, 2, 0):
            for k in (2, 1, 3, 0):
                if chips or k:
                    peer = (me // 4 + chips) % 4 * 4 + (me + k) % 4
                    yield peer, block * MEMBERS + peer

    learn(0)
    learn(1)
    for peer, device in members():
        copy = pair(log_send.at[peer // 4], log_recv.at[me], sem_l, device)
        copy.start()
    log_recv[me] = log_send[me // 4]

    conv_kq = jnp.concatenate([conv_k[...], conv_q[...]], axis=1)
    for s in range(seqs):
        x_sum = x_pad[s, 5:69, :] * conv_x[0:1, :]
        kq_sum = kq_pad[s, 5:69, :] * conv_kq[0:1, :]
        for k in range(1, 4):
            x_sum = x_sum + x_pad[s, 5 + k : 69 + k, :] * conv_x[k : k + 1, :]
            kq_sum = kq_sum + kq_pad[s, 5 + k : 69 + k, :] * conv_kq[k : k + 1, :]
        scaled = silu(x_sum) * step_s[s]
        kq = silu(kq_sum)
        xs_s[s] = scaled
        kq_s[s] = kq
        cum = cum_s[s]
        x_high, x_low = two_parts(scaled * jnp.exp(cum[63:64, :] - cum))
        k_high, k_low = two_parts(kq[:, 0:64])
        state = dot(
            jnp.concatenate([k_high, k_high, k_low], axis=0),
            jnp.concatenate([x_high, x_low, x_high], axis=0),
            ((0,), (0,)),
        )
        for q in range(4):
            chunk_send[s * 4 + q] = state[q * 16 : q * 16 + 16, :].astype(BF16)

    for peer, device in members():
        copy = pair(chunk_send.at[peer], chunk_recv.at[me], sem_c, device)
        copy.start()
    chunk_recv[me] = chunk_send[me]

    for s in range(seqs):
        cum, kq, scaled = cum_s[s], kq_s[s], xs_s[s]
        keys, queries = kq[:, 0:64], kq[:, 64:128]
        query_s[s] = jnp.concatenate(two_parts(queries), axis=1)
        cum_row = jnp.sum(jnp.where(diagonal, cum, 0.0), axis=0, keepdims=True)
        decay = jnp.where(causal, jnp.exp(jnp.where(causal, cum - cum_row, 0.0)), 0.0)
        scores = dot(queries, jnp.concatenate([keys, keys], axis=0), ((1,), (1,)), PRECISE)
        apart = jnp.concatenate(
            [jnp.where(first_head, scaled, 0.0), jnp.where(first_head, 0.0, scaled)], axis=0
        )
        inner_s[s] = dot(scores * decay, apart, precision=PRECISE)
        cum_s[s] = jnp.exp(cum)
        gate_s[s] = silu(gate_s[s])

    def logs_here():
        all_done(log_recv.at[pl.ds(0, MEMBERS - 1)], sem_l.at[1])

    def chunks_here():
        all_done(chunk_recv.at[pl.ds(0, MEMBERS - 1)], sem_c.at[1])

    def far_log(k, device):
        return pair(total_log, total_log_recv.at[k - 1], sem_tl, device)

    def far(k, device):
        return pair(total_send, total_recv.at[k - 1], sem_t, device)

    def later_blocks(act):
        for k in sorted(range(1, blocks), key=lambda k: abs(2 * k - blocks)):
            @pl.when(block + k < blocks)
            def _():
                act(k, sp + k * MEMBERS)

    def count_done(count, side):
        for k in range(1, blocks):
            @pl.when(count == k)
            def _():
                all_done(total_log_recv.at[pl.ds(0, k)], sem_tl.at[side])
                all_done(total_recv.at[pl.ds(0, k)], sem_t.at[side])

    def rows_sent():
        all_done(rows_in.at[pl.ds(0, 7)], sem_gs.at[0])

        @pl.when(has_tail)
        def _():
            for k in range(3):
                tail(k, tail_out, sp=sp + 1, tp=7).wait_send()

        @pl.when((sp > 0) & (core == 1))
        def _():
            tail(4, tail_in, tp=partner).wait_send()

            @pl.when(chip == 0)
            def _():
                tail(3, tail_in, tp=ahead).wait_send()

    rows_sent()

    logs_here()
    log_sum = jnp.zeros((1, 128), F32)
    for m in range(MEMBERS):
        part_logs[m] = jnp.exp(log_sum)
        log_sum = log_sum + log_recv[m]
        log_recv[m] = jnp.exp(log_recv[m])
    total_log[...] = log_sum
    chunks_here()
    running = jnp.zeros((16, 128), F32)
    for m in range(MEMBERS):
        part_sums[m] = running
        running = log_recv[m] * running + chunk_recv[m].astype(F32)
    total_send[...] = running.astype(BF16)
    relay(2)
    learn(2)

    def send_far(k, device):
        far_log(k, device).start()
        far(k, device).start()

    later_blocks(send_far)

    def totals_here():
        count_done(block, 1)

    totals_here()
    incoming = jnp.zeros((16, 128), F32)
    for k in range(blocks - 1, 0, -1):
        incoming = jnp.exp(total_log_recv[k - 1]) * incoming + total_recv[k - 1].astype(F32)
    for m in range(MEMBERS):
        back_send[m] = (part_sums[m] + part_logs[m] * incoming).astype(BF16)
    for peer, device in members():
        copy = pair(back_send.at[peer], back_recv.at[me], sem_b, device)
        copy.start()
    back_recv[me] = back_send[me]

    def parts_sent():
        all_done(log_recv.at[pl.ds(0, MEMBERS - 1)], sem_l.at[0])
        all_done(chunk_recv.at[pl.ds(0, MEMBERS - 1)], sem_c.at[0])
        all_done(back_recv.at[pl.ds(0, MEMBERS - 1)], sem_b.at[0])
        count_done(blocks - 1 - block, 0)

    parts_sent()

    def states_here():
        all_done(back_recv.at[pl.ds(0, MEMBERS - 1)], sem_b.at[1])

    states_here()

    mixed = []
    for s in range(seqs):
        state = back_recv[s * 4 : s * 4 + 4].reshape(64, 128)
        carried = dot(query_s[s], jnp.concatenate([state, state], axis=0))
        gated = (inner_s[s] + carried * cum_s[s]) * gate_s[s]
        mean_sq = jnp.mean(gated * gated, axis=-1, keepdims=True)
        mixed.append(gated * lax.rsqrt(mean_sq + NORM_EPS) * out_gain[...])
    for t in range(8):
        mix_send[t] = jnp.concatenate(
            [part[t * 8 : t * 8 + 8, :] for part in mixed], axis=0
        ).astype(BF16)

    def columns(source):
        return out_ref.at[:, pl.ds(pl.multiple_of(source * 128, 128), 128)]

    for chips in (2, 1, 3, 0):
        for same in (True, False):
            if chips or not same:
                peer = (chip + chips) % 4 * 2 + (core if same else 1 - core)
                remote(
                    mix_send.at[peer], columns(tp), sem_m.at[0], sem_m.at[1], tp=peer
                ).start()
    own = pltpu.make_async_copy(mix_send.at[tp], columns(tp), sem_m.at[2])
    own.start()

    def heads_here():
        all_done(mix_send.at[pl.ds(0, 7)], sem_m.at[1])

    heads_here()
    def heads_sent():
        own.wait()
        all_done(mix_send.at[pl.ds(0, 7)], sem_m.at[0])

    heads_sent()


def body(
    tokens, in_gain, gate_weight, input_weight, key_weight, query_weight, step_weight,
    conv_input, conv_key, conv_query, step_bias, decay_rate, decay_extra, out_gain, out_weight,
):
    places = lax.axis_size("sp")
    blocks = places // MEMBERS
    seqs, _, width = tokens.shape
    inner = out_weight.shape[0]
    local = (seqs, 64, 128)
    padded = (seqs, 72, 128)
    dma = pltpu.SemaphoreType.DMA
    vmem = pltpu.VMEM
    operands = (
        tokens, in_gain.reshape(1, width), gate_weight, input_weight, key_weight.T,
        query_weight.T, step_weight.T, conv_input, conv_key, conv_query,
        step_bias.reshape(1, 2), decay_rate.reshape(1, 2), decay_extra,
        out_gain.reshape(1, 128),
    )
    rows = pl.pallas_call(
        functools.partial(mixer_kernel, places, seqs),
        out_shape=jax.ShapeDtypeStruct((seqs * 8, inner), BF16),
        in_specs=[pl.BlockSpec(memory_space=pl.ANY)] * 14,
        out_specs=pl.BlockSpec(memory_space=pl.ANY),
        scratch_shapes=[
            vmem(tokens.shape, BF16),
            vmem((1, width), F32),
            vmem((width, 256), BF16),
            vmem((256, width), BF16),
            vmem((16, width), BF16),
            vmem(conv_input.shape, F32),
            vmem(conv_key.shape, F32),
            vmem(conv_query.shape, F32),
            vmem((1, 2), F32),
            vmem((1, 2), F32),
            vmem(decay_extra.shape, F32),
            vmem((1, 128), F32),
            vmem((8, seqs * 8, width), BF16),
            vmem((seqs * 4, width), BF16),
            vmem((seqs * 4, width), BF16),
            vmem(local, F32),
            vmem(padded, F32),
            vmem(padded, F32),
            vmem(local, F32),
            vmem(local, F32),
            vmem(local, F32),
            vmem(local, F32),
            vmem(local, F32),
            vmem(local, F32),
            vmem(local, BF16),
            vmem((MEMBERS, 16, 128), BF16),
            vmem((MEMBERS, 16, 128), BF16),
            vmem((seqs, 1, 128), F32),
            vmem((MEMBERS, 1, 128), F32),
            vmem((MEMBERS, 16, 128), F32),
            vmem((MEMBERS, 1, 128), F32),
            vmem((16, 128), BF16),
            vmem((1, 128), F32),
            vmem((blocks - 1, 16, 128), BF16),
            vmem((blocks - 1, 1, 128), F32),
            vmem((MEMBERS, 16, 128), BF16),
            vmem((MEMBERS, 16, 128), BF16),
            vmem((8, seqs * 8, 128), BF16),
            dma((12,)),
            dma((1,)),
            dma((14,)),
            dma((6,)),
            dma((2,)),
            dma((2,)),
            dma((2,)),
            dma((2,)),
            dma((2,)),
            dma((3,)),
            pltpu.SemaphoreType.REGULAR((4,)),
        ],
        compiler_params=pltpu.CompilerParams(
            collective_id=0, has_side_effects=True, vmem_limit_bytes=16 * 2**20
        ),
        cost_estimate=pl.CostEstimate(
            flops=4 * 10**9, bytes_accessed=2 * 2**20, transcendentals=0
        ),
        name="mixer",
    )(*[pltpu.with_memory_space_constraint(operand, pltpu.HBM) for operand in operands])
    result = jnp.dot(rows, out_weight, preferred_element_type=F32)
    return result.astype(BF16).reshape(tokens.shape)


def solution(mesh):
    placed = (
        P(None, ("sp", "tp"), None),
        P(),
        P(None, "tp"),
        P(None, "tp"),
        P(None, "tp"),
        P(None, "tp"),
        P(),
        P(None, "tp"),
        P(None, "tp"),
        P(None, "tp"),
        P("tp"),
        P("tp"),
        P(None, "tp", "sp"),
        P("tp"),
        P(),
    )
    return jax.shard_map(
        body, mesh=mesh, in_specs=placed, out_specs=P(None, ("sp", "tp"), None), check_vma=False
    )
```
